768 devices in a mesh: sp: 96 (over z, y), tp: 8 (over x, core).
Axes of the slice: x: 4, y: 8, z: 12, core: 2. Of those that a mesh axis runs over, the one named last changes fastest.
Arguments:
- tokens: bfloat16 [24576, 2048], P('sp'), may hold values from -72 to 72
- query_weight: bfloat16 [3, 2048, 1024], P(None, None, 'tp'), may hold values from -0.125 to 0.125
- key_weight: bfloat16 [3, 2048, 1024], P(None, None, 'tp'), may hold values from -0.125 to 0.125
- value_weight: bfloat16 [3, 2048, 1024], P(None, None, 'tp'), may hold values from -0.125 to 0.125
- out_weight: bfloat16 [1024, 2048], P(None, 'tp'), may hold values from -2 to 2
Outputs:
- mixed: bfloat16 [24576, 2048], P('sp', 'tp')
The draws below stay inside these ranges and needn't reach their ends.
All inputs are finite; a program needn't handle non-finite values.
Results may differ from the reference program's by a relative error of at most 0.012.
Values may be sent and summed in bfloat16 or wider, within the bound.
No kernel may reach another device: no remote copies, remote signals or barrier semaphores. Data moves between devices by JAX's collectives and lax.ppermute only.
A program may use at most 64 MiB of HBM per device.

```python
import math
import jax
import jax.numpy as jnp
from jax import lax

D = 2048
SLOTS = 16
HEAD_DIM = 64
SIDE_STEPS = 64
MIDDLE_DILATION = 4
FAR_DILATION = 16
HW = 1024
TOKENS = 24576


def draw_tokens(key, part):
    base = jnp.clip(jax.random.normal(key, (TOKENS, D), jnp.float32), -6.0, 6.0)
    return base.astype(jnp.bfloat16)


def shard_levels(stream_key, extent, cuts, low, high):
    def one(position, blocks):
        draws = jax.random.uniform(jax.random.fold_in(jax.random.fold_in(stream_key, 6), position), (blocks,), jnp.float32, low / len(cuts), high / len(cuts))
        return jnp.repeat(jnp.exp(draws), extent[position] // blocks).reshape((-1,) + (1,) * (len(extent) - position - 1))

    level = one(*cuts[0])
    for cut in cuts[1:]:
        level = level * one(*cut)
    return level


def centred(rng, shape, spread, limit, pieces=(), kind=jnp.bfloat16):
    values = jax.random.normal(rng, shape, jnp.float32) * spread
    if len(pieces) > 0:
        values = shard_levels(rng, shape, pieces, -0.22, 0.18) * values
    return jnp.clip(values, min=-limit, max=limit).astype(kind)


def setup_inputs(seed: int = 0) -> dict:
    seeds = jax.random.split(jax.random.key(seed), 6)
    return {
        "tokens": draw_tokens(jax.random.fold_in(seeds[5], 71), 0),
        "query_weight": centred(seeds[1], (3, D, HW), D ** -0.5, 0.125, ((2, 8),)),
        "key_weight": centred(seeds[2], (3, D, HW), D ** -0.5, 0.125, ((2, 8),)),
        "value_weight": centred(seeds[3], (3, D, HW), D ** -0.5, 0.125, ((2, 8),)),
        "out_weight": centred(seeds[4], (HW, D), (HW // 128) ** -0.5, 2.0, ((1, 8),)),
    }


def rotate(projected, offset_pos):
    length, columns = projected.shape
    heads = columns // HEAD_DIM
    half = HEAD_DIM // 2
    positions = (offset_pos + jnp.arange(length)).astype(jnp.float32)
    inverse = 1.0 / (10000.0 ** (jnp.arange(half, dtype=jnp.float32) * 2.0 / HEAD_DIM))
    angles = positions[:, None] * inverse[None, :]
    angles = jnp.concatenate([angles, angles], axis=-1)
    cosine_table = jnp.cos(angles)[:, None, :]
    sine = jnp.sin(angles)[:, None, :]
    shaped = projected.reshape(length, heads, HEAD_DIM)
    turned = jnp.concatenate([-shaped[..., half:], shaped[..., :half]], axis=-1)
    return (shaped * cosine_table + turned * sine).reshape(length, columns)


def banded(queries, key_ext, value_ext, dilation, offset_pos, seq_len):
    length, columns = queries.shape
    heads = columns // HEAD_DIM
    class_len = length // dilation
    block_len = math.gcd(SIDE_STEPS, class_len)
    blocks = class_len // block_len
    extra = 2 * SIDE_STEPS // block_len
    query_blocks = queries.reshape(blocks, block_len, dilation, heads, HEAD_DIM)
    key_blocks = key_ext.reshape(blocks + extra, block_len, dilation, heads, HEAD_DIM)
    value_blocks = value_ext.reshape(blocks + extra, block_len, dilation, heads, HEAD_DIM)
    key_win = jnp.concatenate([key_blocks[shift_idx:shift_idx + blocks] for shift_idx in range(extra + 1)], axis=1)
    value_win = jnp.concatenate([value_blocks[shift_idx:shift_idx + blocks] for shift_idx in range(extra + 1)], axis=1)
    scores = jnp.einsum('bqrhe,bkrhe->brhqk', query_blocks.astype(jnp.float32), key_win.astype(jnp.float32))
    scores = scores * (HEAD_DIM ** -0.5)
    width_keys = key_win.shape[1]
    relative = jnp.arange(width_keys)[None, :] - jnp.arange(block_len)[:, None]
    within = (relative >= 0) & (relative <= 2 * SIDE_STEPS)
    key_rows = jnp.arange(blocks)[:, None] * block_len + jnp.arange(width_keys)[None, :]
    spots = offset_pos - SIDE_STEPS * dilation + dilation * key_rows[:, :, None] + jnp.arange(dilation)[None, None, :]
    inside = (spots >= 0) & (spots < seq_len)
    allowed = within[None, None, None] & jnp.transpose(inside, (0, 2, 1))[:, :, None, None, :]
    scores = jnp.where(allowed, scores, -1e30)
    row_max = jnp.max(scores, axis=-1, keepdims=True)
    expo = jnp.exp(scores - row_max)
    denom = jnp.sum(expo, axis=-1)
    probs = lax.optimization_barrier(expo.astype(jnp.bfloat16))
    summed = jnp.einsum('brhqk,bkrhe->bqrhe', probs.astype(jnp.float32), value_win.astype(jnp.float32))
    group_out = summed / jnp.transpose(denom, (0, 3, 1, 2))[..., None]
    log_sum = row_max[..., 0] + jnp.log(denom)
    log_sum = jnp.transpose(log_sum, (0, 3, 1, 2)).reshape(length, heads)
    return group_out.reshape(length, columns), log_sum


def reference(tokens, query_weight, key_weight, value_weight, out_weight):
    seq_len = tokens.shape[0]
    group_dilations = (1, MIDDLE_DILATION, FAR_DILATION)
    outputs = []
    log_sums = []
    for group_idx in range(3):
        queries = rotate(jnp.dot(tokens, query_weight[group_idx], preferred_element_type=jnp.float32), 0).astype(jnp.bfloat16)
        keys_all = rotate(jnp.dot(tokens, key_weight[group_idx], preferred_element_type=jnp.float32), 0).astype(jnp.bfloat16)
        value_rows_full = jnp.dot(tokens, value_weight[group_idx], preferred_element_type=jnp.float32).astype(jnp.bfloat16)
        reach = SIDE_STEPS * group_dilations[group_idx]
        key_ext = jnp.pad(keys_all, ((reach, reach), (0, 0)))
        value_ext = jnp.pad(value_rows_full, ((reach, reach), (0, 0)))
        group_out, log_sum = banded(queries, key_ext, value_ext, group_dilations[group_idx], 0, seq_len)
        outputs.append(group_out)
        log_sums.append(log_sum)
    merge_w = jax.nn.softmax(jnp.stack(log_sums, axis=0), axis=0)
    stacked = jnp.stack(outputs, axis=0).reshape(3, seq_len, SLOTS, HEAD_DIM)
    merged = jnp.sum(merge_w[..., None] * stacked, axis=0).reshape(seq_len, HW).astype(jnp.bfloat16)
    return jnp.dot(merged, out_weight, preferred_element_type=jnp.float32).astype(jnp.bfloat16)
```

```python
import functools

import jax
import jax.numpy as jnp
import numpy as np
from jax import lax
from jax.experimental import pallas as pl
from jax.experimental.pallas import tpu as pltpu
from jax.sharding import PartitionSpec as P

HEAD_DIM = 64
SIDE = 64
MIDDLE = 4
FAR = 16
LANES = 128
ROW = 8
BF = jnp.bfloat16
F32 = jnp.float32
SPLIT = 4


def rotary_tables(devices, length):
    lane = np.arange(LANES)
    inverse = 10000.0 ** (-2.0 * (lane % (HEAD_DIM // 2)) / HEAD_DIM)
    sign = np.where(lane % HEAD_DIM < HEAD_DIM // 2, -1.0, 1.0)
    base = np.arange(devices)[:, None] * length * inverse[None]
    step = np.arange(length)[:, None] * inverse[None]
    far = np.concatenate([np.cos(base), np.sin(base), sign * np.cos(base), sign * np.sin(base)], axis=1)
    near = np.stack([np.cos(step), np.sin(step)])
    return far.astype(np.float32), near.astype(np.float32)


def turn_tables(far_ref, near_ref):
    row = far_ref[pl.ds(lax.axis_index("sp"), 1), :]
    cos_base, sin_base = row[:, :LANES], row[:, LANES : 2 * LANES]
    scos_base, ssin_base = row[:, 2 * LANES : 3 * LANES], row[:, 3 * LANES :]
    cos_step, sin_step = near_ref[0], near_ref[1]
    return cos_base * cos_step - sin_base * sin_step, ssin_base * cos_step + scos_base * sin_step


def swap_halves(x):
    lane = lax.broadcasted_iota(jnp.int32, x.shape, 1)
    half = HEAD_DIM // 2
    return jnp.where(
        lane % HEAD_DIM < half, pltpu.roll(x, LANES - half, 1), pltpu.roll(x, half, 1)
    )


def rotate(x, tables):
    return x * tables[0] + swap_halves(x) * tables[1]


def store_by_class(x, scratch, out, dilation):
    scratch[...] = x
    n = x.shape[0] // dilation
    for c in range(dilation):
        out[pl.ds(c * n, n), :] = scratch[pl.ds(c, n, stride=dilation), :].astype(BF)


def far_kernel(tok, wk, wv, far, near, out, acc, scratch):
    step = pl.program_id(0)

    @pl.when(step == 0)
    def _():
        acc[...] = jnp.zeros_like(acc)

    x = tok[...]
    acc[0] += jnp.dot(x, wk[0], preferred_element_type=F32)
    acc[1] += jnp.dot(x, wv[0], preferred_element_type=F32)

    @pl.when(step == SPLIT - 1)
    def _():
        tables = turn_tables(far, near)
        store_by_class(rotate(acc[0], tables), scratch.at[0], out.at[0], FAR)
        store_by_class(acc[1], scratch.at[1], out.at[1], FAR)


def rest_kernel(tok, wq, wk, wv, far, near, q3, q12, kv1, up, down, acc, scratch):
    step = pl.program_id(0)

    @pl.when(step == 0)
    def _():
        acc[...] = jnp.zeros_like(acc)

    x = tok[...]
    for g in range(3):
        acc[g] += jnp.dot(x, wq[g], preferred_element_type=F32)
    for g in range(2):
        acc[3 + g] += jnp.dot(x, wk[g], preferred_element_type=F32)
        acc[5 + g] += jnp.dot(x, wv[g], preferred_element_type=F32)

    @pl.when(step == SPLIT - 1)
    def _():
        length = tok.shape[0]
        tables = turn_tables(far, near)
        store_by_class(rotate(acc[2], tables), scratch.at[0], q3, FAR)
        q12[0] = rotate(acc[0], tables).astype(BF)
        store_by_class(rotate(acc[1], tables), scratch.at[1], q12.at[1], MIDDLE)
        k1 = rotate(acc[3], tables).astype(BF)
        v1 = acc[5].astype(BF)
        for n, x1 in enumerate((k1, v1)):
            kv1[n] = x1
            up[n, pl.ds(length, SIDE), :] = x1[length - SIDE :]
            down[n, pl.ds(length, SIDE), :] = x1[:SIDE]
        middle = (rotate(acc[4], tables), acc[6])
        for n in range(2):
            scratch[2 + n] = middle[n]
            rows = length // MIDDLE
            for c in range(MIDDLE):
                part = scratch[2 + n, pl.ds(c, rows, stride=MIDDLE), :].astype(BF)
                up[n, pl.ds(c * rows, rows), :] = part
                down[n, pl.ds(c * rows, rows), :] = part


def attend(q, k, v, low, high):
    n, keys = q.shape[0], k.shape[0]
    lane = lax.broadcasted_iota(jnp.int32, (1, LANES), 1)
    first = (lane < HEAD_DIM).astype(F32).astype(BF)
    second = (lane >= HEAD_DIM).astype(F32).astype(BF)
    both = jnp.concatenate([q * first, q * second], axis=0)
    scores = lax.dot_general(both, k, (((1,), (1,)), ((), ())), preferred_element_type=F32)
    scores = scores * HEAD_DIM ** (-0.5)
    column = lax.broadcasted_iota(jnp.int32, (n, keys), 1)
    relative = column - lax.broadcasted_iota(jnp.int32, (n, keys), 0)
    allowed = (relative >= 0) & (relative <= 2 * SIDE) & (column >= low) & (column < high)
    outs, tops, sums = [], [], []
    for head in range(2):
        part = jnp.where(allowed, scores[head * n : (head + 1) * n], -1e30)
        top = jnp.max(part, axis=-1, keepdims=True)
        expo = jnp.exp(part - top)
        sums.append(jnp.sum(expo, axis=-1, keepdims=True))
        tops.append(top)
        outs.append(jnp.dot(expo.astype(BF), v, preferred_element_type=F32))
    is_first = lax.broadcasted_iota(jnp.int32, (n, LANES), 1) < HEAD_DIM
    denom = jnp.where(is_first, sums[0], sums[1])
    top = jnp.where(is_first, tops[0], tops[1])
    return jnp.where(is_first, outs[0], outs[1]) / denom, top + jnp.log(denom)


def merge(out_a, lse_a, out_b, lse_b):
    top = jnp.maximum(lse_a, lse_b)
    wa, wb = jnp.exp(lse_a - top), jnp.exp(lse_b - top)
    total = wa + wb
    return (wa * out_a + wb * out_b) / total, top + jnp.log(total)


def near_attention_kernel(devices, q12, kv1, up, low, high, out, lse, out2, lse2):
    length = kv1.shape[1]
    me = lax.axis_index("sp")
    rows = length // MIDDLE
    start = jnp.where(me == 0, SIDE, 0)
    for c in range(MIDDLE):
        at = pl.ds(c * rows, rows)
        k = jnp.concatenate([low[0, at, :], up[0, at, :], high[0, at, :]], axis=0)
        v = jnp.concatenate([low[1, at, :], up[1, at, :], high[1, at, :]], axis=0)
        o, l = attend(
            q12[1, at, :], k, v, start, jnp.where(me == devices - 1, 2 * rows, 3 * rows)
        )
        out2[pl.ds(c, rows, stride=MIDDLE), :] = o
        lse2[pl.ds(c, rows, stride=MIDDLE), :] = l
    block = 2 * SIDE
    for b in range(length // block):
        ks, vs = [], []
        for n, xs in enumerate((ks, vs)):
            if b == 0:
                xs.append(low[n, pl.ds(length, SIDE), :])
            first = max(b * block - SIDE, 0)
            last = min((b + 1) * block + SIDE, length)
            xs.append(kv1[n, pl.ds(first, last - first), :])
            if b == length // block - 1:
                xs.append(high[n, pl.ds(length, SIDE), :])
        at = pl.ds(b * block, block)
        o, l = attend(
            q12[0, at, :],
            jnp.concatenate(ks, axis=0),
            jnp.concatenate(vs, axis=0),
            start if b == 0 else 0,
            jnp.where(me == devices - 1, block + SIDE, 2 * block)
            if b == length // block - 1
            else 2 * block,
        )
        out[at, :], lse[at, :] = merge(o, l, out2[at, :], lse2[at, :])


def far_attention_kernel(rows_of_devices, parts, out):
    z = lax.axis_index("sp") // ROW
    low = jnp.where(z == 0, SIDE, 0)
    size = parts.shape[1] // 5
    run = size // 2
    half = ROW // 2
    queries = ROW * run
    high = jnp.where(z == rows_of_devices - 1, queries + SIDE, queries + 2 * SIDE)
    lane = lax.broadcasted_iota(jnp.int32, (queries, LANES), 1)
    for e in range(2):
        piece = lambda a, y: parts[y, pl.ds(a * size + e * run, run), :]
        q = jnp.concatenate([piece(0, y) for y in range(ROW)], axis=0)
        kv = [
            jnp.concatenate(
                [piece(a + 2, y) for y in range(half, ROW)]
                + [piece(a, y) for y in range(ROW)]
                + [piece(a + 2, y) for y in range(half)],
                axis=0,
            )
            for a in (1, 2)
        ]
        o, l = attend(q, kv[0], kv[1], low, high)
        coarse = l.astype(BF).astype(F32)
        l = jnp.where(lane % HEAD_DIM < HEAD_DIM // 2, coarse, l - coarse).astype(BF)
        o = o.astype(BF)
        for y in range(ROW):
            out[y, pl.ds(e * run, run), :] = o[y * run : (y + 1) * run]
            out[y, pl.ds(size + e * run, run), :] = l[y * run : (y + 1) * run]


def merge_kernel(parts, out12, lse12, merged, out3, lse3):
    size = parts.shape[1] // 2
    run = size // 2
    for c in range(FAR):
        y, e = c // 2, c % 2
        at = pl.ds(c, run, stride=FAR)
        out3[at, :] = parts[y, pl.ds(e * run, run), :].astype(F32)
        lse3[at, :] = parts[y, pl.ds(size + e * run, run), :].astype(F32)
    l = lse3[...]
    o, _ = merge(out12[...], lse12[...], out3[...], l + swap_halves(l))
    merged[...] = o.astype(BF)


def vmem(shape):
    return jax.ShapeDtypeStruct(shape, BF)


def whole():
    return pl.BlockSpec(memory_space=pltpu.VMEM)


def cost(flops, size):
    return pl.CostEstimate(flops=flops, bytes_accessed=size, transcendentals=0)


def per_device(devices, tokens, query_weight, key_weight, value_weight, out_weight):
    length, width = tokens.shape
    columns = key_weight.shape[2]
    far, near = rotary_tables(devices, length)
    chunk = width // SPLIT
    fixed = [
        pl.BlockSpec(far.shape, lambda k: (0, 0)),
        pl.BlockSpec(near.shape, lambda k: (0, 0, 0)),
    ]
    token_spec = pl.BlockSpec((length, chunk), lambda k: (0, k))
    one = pl.BlockSpec((1, chunk, columns), lambda k: (2, k, 0))
    kv3 = pl.pallas_call(
        far_kernel,
        grid=(SPLIT,),
        in_specs=[token_spec, one, one] + fixed,
        out_specs=pl.BlockSpec((2, length, columns), lambda k: (0, 0, 0)),
        out_shape=vmem((2, length, columns)),
        scratch_shapes=[
            pltpu.VMEM((2, length, columns), F32),
            pltpu.VMEM((2, length, columns), F32),
        ],
        cost_estimate=cost(4 * length * width * columns, 2 << 20),
        name="far_keys_values",
    )(tokens, key_weight, value_weight, far, near)

    half = ROW // 2
    route = []
    for s in range(devices):
        target = s + ROW if s % ROW >= half else s - ROW
        if 0 <= target < devices:
            route.append((s, target))
    halo3 = lax.ppermute(kv3, "sp", route)

    two = pl.BlockSpec((2, chunk, columns), lambda k: (0, k, 0))
    edge = length + SIDE
    shapes = [
        (length, columns),
        (2, length, columns),
        (2, length, columns),
        (2, edge, columns),
        (2, edge, columns),
    ]
    q3, q12, kv1, up, down = pl.pallas_call(
        rest_kernel,
        grid=(SPLIT,),
        in_specs=[token_spec, pl.BlockSpec((3, chunk, columns), lambda k: (0, k, 0)), two, two]
        + fixed,
        out_specs=[
            pl.BlockSpec(s, functools.partial(lambda n, k: (0,) * n, len(s))) for s in shapes
        ],
        out_shape=[vmem(s) for s in shapes],
        scratch_shapes=[
            pltpu.VMEM((7, length, columns), F32),
            pltpu.VMEM((4, length, columns), F32),
        ],
        cost_estimate=cost(14 * length * width * columns, 5 << 20),
        name="projections",
    )(tokens, query_weight, key_weight, value_weight, far, near)

    low = lax.ppermute(up, "sp", [(s, s + 1) for s in range(devices - 1)])
    high = lax.ppermute(down, "sp", [(s + 1, s) for s in range(devices - 1)])

    size = length // ROW
    packed = jnp.concatenate([q3[None], kv3, halo3], axis=0).reshape(5, ROW, size, columns)
    packed = jnp.swapaxes(packed, 0, 1).reshape(ROW, 5 * size, columns)
    groups = [[z * ROW + y for y in range(ROW)] for z in range(devices // ROW)]
    parts = lax.all_to_all(packed, "sp", 0, 0, axis_index_groups=groups, tiled=True)

    back = pl.pallas_call(
        functools.partial(far_attention_kernel, devices // ROW),
        in_specs=[whole()],
        out_specs=whole(),
        out_shape=vmem((ROW, 2 * size, columns)),
        cost_estimate=cost(1 << 27, 1 << 19),
        name="far_attention",
    )(parts)
    parts3 = lax.all_to_all(back, "sp", 0, 0, axis_index_groups=groups, tiled=True)

    flat = jax.ShapeDtypeStruct((length, columns), F32)
    out12, lse12 = pl.pallas_call(
        functools.partial(near_attention_kernel, devices),
        in_specs=[whole()] * 5,
        out_specs=[whole()] * 2,
        out_shape=[flat, flat],
        scratch_shapes=[pltpu.VMEM((length, columns), F32)] * 2,
        cost_estimate=cost(1 << 28, 1 << 20),
        name="near_attention",
    )(q12, kv1, up, low, high)

    merged = pl.pallas_call(
        merge_kernel,
        in_specs=[whole()] * 3,
        out_specs=whole(),
        out_shape=vmem((length, columns)),
        scratch_shapes=[pltpu.VMEM((length, columns), F32)] * 2,
        cost_estimate=cost(1 << 20, 1 << 19),
        name="merge",
    )(parts3, out12, lse12)

    gathered = lax.all_gather(merged, "tp", axis=0, tiled=False)
    gathered = jnp.swapaxes(gathered, 0, 1).reshape(length, -1)
    mixed = jnp.dot(gathered, out_weight, preferred_element_type=F32)
    return mixed.astype(BF)


def solution(mesh):
    weights = P(None, None, "tp")
    return jax.shard_map(
        functools.partial(per_device, mesh.shape["sp"]),
        mesh=mesh,
        in_specs=(P("sp", None), weights, weights, weights, P(None, "tp")),
        out_specs=P("sp", "tp"),
        check_vma=False,
    )
```

```python
import functools

import jax
import jax.numpy as jnp
import numpy as np
from jax import lax
from jax.experimental import pallas as pl
from jax.experimental.pallas import tpu as pltpu
from jax.sharding import PartitionSpec as P


HEAD_DIM = 64
SIDE = 64
MIDDLE = 4
FAR = 16
LANES = 128
ROW = 8
BF = jnp.bfloat16
F32 = jnp.float32
PIECES = 2


def rotary_tables(devices, length):
    lane = np.arange(LANES)
    inverse = 10000.0 ** (-2.0 * (lane % (HEAD_DIM // 2)) / HEAD_DIM)
    sign = np.where(lane % HEAD_DIM < HEAD_DIM // 2, -1.0, 1.0)
    base = np.arange(devices)[:, None] * length * inverse[None]
    step = np.arange(length)[:, None] * inverse[None]
    far = np.concatenate([np.cos(base), np.sin(base), sign * np.cos(base), sign * np.sin(base)], axis=1)
    near = np.stack([np.cos(step), np.sin(step)])
    return far.astype(np.float32), near.astype(np.float32)


def turn_tables(far_ref, near_ref):
    row = far_ref[pl.ds(lax.axis_index("sp"), 1), :]
    cos_base, sin_base = row[:, :LANES], row[:, LANES : 2 * LANES]
    scos_base, ssin_base = row[:, 2 * LANES : 3 * LANES], row[:, 3 * LANES :]
    cos_step, sin_step = near_ref[0], near_ref[1]
    return cos_base * cos_step - sin_base * sin_step, ssin_base * cos_step + scos_base * sin_step


def swap_halves(x):
    lane = lax.broadcasted_iota(jnp.int32, x.shape, 1)
    half = HEAD_DIM // 2
    return jnp.where(
        lane % HEAD_DIM < half, pltpu.roll(x, LANES - half, 1), pltpu.roll(x, half, 1)
    )


def rotate(x, tables):
    return x * tables[0] + swap_halves(x) * tables[1]


def store_by_class(x, scratch, out, dilation):
    scratch[...] = x
    n = x.shape[0] // dilation
    for c in range(dilation):
        out[pl.ds(c * n, n), :] = scratch[pl.ds(c, n, stride=dilation), :].astype(BF)


def fetch(tok, tok_buf, weights, buf, sem):
    width = tok.shape[1] // PIECES
    rows = buf.shape[0] // PIECES
    copies = []
    for p in range(PIECES):
        at = pl.ds(p * width, width)
        copies.append(pltpu.make_async_copy(tok.at[:, at], tok_buf.at[:, at], sem.at[p]))
        copies[-1].start()
        if p == 0:
            for n, (ref, group) in enumerate(weights[:2]):
                for q in range(PIECES):
                    part = pl.ds(q * rows, rows)
                    copy = pltpu.make_async_copy(
                        ref.at[group, part, :],
                        buf.at[part, pl.ds(n * LANES, LANES)],
                        sem.at[PIECES + n * PIECES + q],
                    )
                    copies.append(copy)
    for q in range(PIECES):
        for n in range(2):
            copies[1 + n * PIECES + q].start()
    rest = []
    for n, (ref, group) in enumerate(weights[2:], 2):
        rest.append(
            pltpu.make_async_copy(
                ref.at[group], buf.at[:, pl.ds(n * LANES, LANES)], sem.at[PIECES * 3 + n - 2]
            )
        )
        rest[-1].start()
    tokens = [copies[0]] + copies[1 + 2 * PIECES :]
    return tokens, [[copies[1 + n * PIECES + q] for n in range(2)] for q in range(PIECES)], rest


def first_pair(tok_buf, buf, copies):
    tokens, pair, _ = copies
    total = None
    width = tok_buf.shape[1] // PIECES
    for p in range(PIECES):
        tokens[p].wait()
        for copy in pair[p]:
            copy.wait()
        at = pl.ds(p * width, width)
        part = jnp.dot(tok_buf[:, at], buf[at, : 2 * LANES], preferred_element_type=F32)
        total = part if total is None else total + part
    return total


def far_kernel(tok, wk, wv, far, near, out, tok_buf, buf, scratch, sem):
    copies = fetch(tok, tok_buf, ((wk, 2), (wv, 2)), buf, sem)
    tables = turn_tables(far, near)
    both = first_pair(tok_buf, buf, copies)
    store_by_class(rotate(both[:, :LANES], tables), scratch.at[0], out.at[0], FAR)
    store_by_class(both[:, LANES:], scratch.at[1], out.at[1], FAR)


def rest_kernel(
    tok, wq, wk, wv, far, near, q3, q12, kv1, up, down, tok_buf, buf, scratch, sem
):
    length = tok.shape[0]
    weights = ((wk, 1), (wv, 1), (wk, 0), (wv, 0), (wq, 2), (wq, 1), (wq, 0))
    copies = fetch(tok, tok_buf, weights, buf, sem)
    tables = turn_tables(far, near)
    both = first_pair(tok_buf, buf, copies)
    rest = copies[2]
    rows = length // MIDDLE
    for n, x2 in enumerate((rotate(both[:, :LANES], tables), both[:, LANES:])):
        scratch[n] = x2
        for c in range(MIDDLE):
            part = scratch[n, pl.ds(c, rows, stride=MIDDLE), :].astype(BF)
            up[n, pl.ds(c * rows, rows), :] = part
            down[n, pl.ds(c * rows, rows), :] = part
    x = tok_buf[...]

    def project(n, count):
        for m in range(count):
            rest[n - 2 + m].wait()
        at = pl.ds(n * LANES, count * LANES)
        return jnp.dot(x, buf[:, at], preferred_element_type=F32)

    both = project(2, 2)
    for n, x1 in enumerate((rotate(both[:, :LANES], tables), both[:, LANES:])):
        x1 = x1.astype(BF)
        kv1[n] = x1
        up[n, pl.ds(length, SIDE), :] = x1[length - SIDE :]
        down[n, pl.ds(length, SIDE), :] = x1[:SIDE]
    both = project(4, 2)
    store_by_class(rotate(both[:, :LANES], tables), scratch.at[2], q3, FAR)
    store_by_class(rotate(both[:, LANES:], tables), scratch.at[3], q12.at[1], MIDDLE)
    q12[0] = rotate(project(6, 1), tables).astype(BF)


def attend(q, k, v, low, high):
    n, keys = q.shape[0], k.shape[0]
    lane = lax.broadcasted_iota(jnp.int32, (1, LANES), 1)
    first = (lane < HEAD_DIM).astype(F32).astype(BF)
    second = (lane >= HEAD_DIM).astype(F32).astype(BF)
    both = jnp.concatenate([q * first, q * second], axis=0)
    scores = lax.dot_general(both, k, (((1,), (1,)), ((), ())), preferred_element_type=F32)
    scores = scores * HEAD_DIM ** (-0.5)
    column = lax.broadcasted_iota(jnp.int32, (n, keys), 1)
    relative = column - lax.broadcasted_iota(jnp.int32, (n, keys), 0)
    allowed = (relative >= 0) & (relative <= 2 * SIDE) & (column >= low) & (column < high)
    outs, tops, sums = [], [], []
    for head in range(2):
        part = jnp.where(allowed, scores[head * n : (head + 1) * n], -1e30)
        top = jnp.max(part, axis=-1, keepdims=True)
        expo = jnp.exp(part - top)
        sums.append(jnp.sum(expo, axis=-1, keepdims=True))
        tops.append(top)
        outs.append(jnp.dot(expo.astype(BF), v, preferred_element_type=F32))
    is_first = lax.broadcasted_iota(jnp.int32, (n, LANES), 1) < HEAD_DIM
    denom = jnp.where(is_first, sums[0], sums[1])
    top = jnp.where(is_first, tops[0], tops[1])
    return jnp.where(is_first, outs[0], outs[1]) / denom, top + jnp.log(denom)


def merge(out_a, lse_a, out_b, lse_b):
    top = jnp.maximum(lse_a, lse_b)
    wa, wb = jnp.exp(lse_a - top), jnp.exp(lse_b - top)
    total = wa + wb
    return (wa * out_a + wb * out_b) / total, top + jnp.log(total)


def near_attention_kernel(devices, q12, kv1, up, low, high, out, lse, out2, lse2):
    length = kv1.shape[1]
    me = lax.axis_index("sp")
    rows = length // MIDDLE
    start = jnp.where(me == 0, SIDE, 0)
    for c in range(MIDDLE):
        at = pl.ds(c * rows, rows)
        k = jnp.concatenate([low[0, at, :], up[0, at, :], high[0, at, :]], axis=0)
        v = jnp.concatenate([low[1, at, :], up[1, at, :], high[1, at, :]], axis=0)
        o, l = attend(
            q12[1, at, :], k, v, start, jnp.where(me == devices - 1, 2 * rows, 3 * rows)
        )
        out2[pl.ds(c, rows, stride=MIDDLE), :] = o
        lse2[pl.ds(c, rows, stride=MIDDLE), :] = l
    block = 2 * SIDE
    for b in range(length // block):
        ks, vs = [], []
        for n, xs in enumerate((ks, vs)):
            if b == 0:
                xs.append(low[n, pl.ds(length, SIDE), :])
            first = max(b * block - SIDE, 0)
            last = min((b + 1) * block + SIDE, length)
            xs.append(kv1[n, pl.ds(first, last - first), :])
            if b == length // block - 1:
                xs.append(high[n, pl.ds(length, SIDE), :])
        at = pl.ds(b * block, block)
        o, l = attend(
            q12[0, at, :],
            jnp.concatenate(ks, axis=0),
            jnp.concatenate(vs, axis=0),
            start if b == 0 else 0,
            jnp.where(me == devices - 1, block + SIDE, 2 * block)
            if b == length // block - 1
            else 2 * block,
        )
        out[at, :], lse[at, :] = merge(o, l, out2[at, :], lse2[at, :])


def far_attention_kernel(rows_of_devices, parts, out):
    z = lax.axis_index("sp") // ROW
    low = jnp.where(z == 0, SIDE, 0)
    size = parts.shape[1] // 5
    run = size // 2
    half = ROW // 2
    queries = ROW * run
    high = jnp.where(z == rows_of_devices - 1, queries + SIDE, queries + 2 * SIDE)
    lane = lax.broadcasted_iota(jnp.int32, (queries, LANES), 1)
    for e in range(2):
        piece = lambda a, y: parts[y, pl.ds(a * size + e * run, run), :]
        q = jnp.concatenate([piece(0, y) for y in range(ROW)], axis=0)
        kv = [
            jnp.concatenate(
                [piece(a + 2, y) for y in range(half, ROW)]
                + [piece(a, y) for y in range(ROW)]
                + [piece(a + 2, y) for y in range(half)],
                axis=0,
            )
            for a in (1, 2)
        ]
        o, l = attend(q, kv[0], kv[1], low, high)
        coarse = l.astype(BF).astype(F32)
        l = jnp.where(lane % HEAD_DIM < HEAD_DIM // 2, coarse, l - coarse).astype(BF)
        o = o.astype(BF)
        for y in range(ROW):
            out[y, pl.ds(e * run, run), :] = o[y * run : (y + 1) * run]
            out[y, pl.ds(size + e * run, run), :] = l[y * run : (y + 1) * run]


def merge_kernel(parts, out12, lse12, merged, out3, lse3):
    size = parts.shape[1] // 2
    run = size // 2
    for c in range(FAR):
        y, e = c // 2, c % 2
        at = pl.ds(c, run, stride=FAR)
        out3[at, :] = parts[y, pl.ds(e * run, run), :].astype(F32)
        lse3[at, :] = parts[y, pl.ds(size + e * run, run), :].astype(F32)
    l = lse3[...]
    o, _ = merge(out12[...], lse12[...], out3[...], l + swap_halves(l))
    merged[...] = o.astype(BF)


def vmem(shape):
    return jax.ShapeDtypeStruct(shape, BF)


def whole():
    return pl.BlockSpec(memory_space=pltpu.VMEM)


def room(mib):
    return pltpu.CompilerParams(vmem_limit_bytes=mib << 20)


def cost(flops, size):
    return pl.CostEstimate(flops=flops, bytes_accessed=size, transcendentals=0)


def per_device(devices, tokens, query_weight, key_weight, value_weight, out_weight):
    length, width = tokens.shape
    columns = key_weight.shape[2]
    far, near = rotary_tables(devices, length)
    hbm = pl.BlockSpec(memory_space=pltpu.HBM)
    kv3 = pl.pallas_call(
        far_kernel,
        in_specs=[hbm, hbm, hbm, whole(), whole()],
        out_specs=whole(),
        out_shape=vmem((2, length, columns)),
        scratch_shapes=[
            pltpu.VMEM((length, width), BF),
            pltpu.VMEM((width, 2 * columns), BF),
            pltpu.VMEM((2, length, columns), F32),
            pltpu.SemaphoreType.DMA((3 * PIECES,)),
        ],
        cost_estimate=cost(4 * length * width * columns, 2 << 20),
        compiler_params=room(63),
        name="far_keys_values",
    )(tokens, key_weight, value_weight, far, near)

    half = ROW // 2
    route = []
    for s in range(devices):
        target = s + ROW if s % ROW >= half else s - ROW
        if 0 <= target < devices:
            route.append((s, target))
    halo3 = lax.ppermute(kv3, "sp", route)

    edge = length + SIDE
    shapes = [
        (length, columns),
        (2, length, columns),
        (2, length, columns),
        (2, edge, columns),
        (2, edge, columns),
    ]
    q3, q12, kv1, up, down = pl.pallas_call(
        rest_kernel,
        in_specs=[hbm, hbm, hbm, hbm, whole(), whole()],
        out_specs=[whole()] * len(shapes),
        out_shape=[vmem(s) for s in shapes],
        scratch_shapes=[
            pltpu.VMEM((length, width), BF),
            pltpu.VMEM((width, 7 * columns), BF),
            pltpu.VMEM((4, length, columns), F32),
            pltpu.SemaphoreType.DMA((3 * PIECES + 5,)),
        ],
        cost_estimate=cost(14 * length * width * columns, 5 << 20),
        compiler_params=room(63),
        name="projections",
    )(tokens, query_weight, key_weight, value_weight, far, near)

    low = lax.ppermute(up, "sp", [(s, s + 1) for s in range(devices - 1)])
    high = lax.ppermute(down, "sp", [(s + 1, s) for s in range(devices - 1)])

    size = length // ROW
    packed = jnp.concatenate([q3[None], kv3, halo3], axis=0).reshape(5, ROW, size, columns)
    packed = jnp.swapaxes(packed, 0, 1).reshape(ROW, 5 * size, columns)
    groups = [[z * ROW + y for y in range(ROW)] for z in range(devices // ROW)]
    parts = lax.all_to_all(packed, "sp", 0, 0, axis_index_groups=groups, tiled=True)

    back = pl.pallas_call(
        functools.partial(far_attention_kernel, devices // ROW),
        in_specs=[whole()],
        out_specs=whole(),
        out_shape=vmem((ROW, 2 * size, columns)),
        cost_estimate=cost(1 << 27, 1 << 19),
        compiler_params=room(4),
        name="far_attention",
    )(parts)
    parts3 = lax.all_to_all(back, "sp", 0, 0, axis_index_groups=groups, tiled=True)

    flat = jax.ShapeDtypeStruct((length, columns), F32)
    out12, lse12 = pl.pallas_call(
        functools.partial(near_attention_kernel, devices),
        in_specs=[whole()] * 5,
        out_specs=[whole()] * 2,
        out_shape=[flat, flat],
        scratch_shapes=[pltpu.VMEM((length, columns), F32)] * 2,
        cost_estimate=cost(1 << 28, 1 << 20),
        compiler_params=room(6),
        name="near_attention",
    )(q12, kv1, up, low, high)

    merged = pl.pallas_call(
        merge_kernel,
        in_specs=[whole()] * 3,
        out_specs=whole(),
        out_shape=vmem((length, columns)),
        scratch_shapes=[pltpu.VMEM((length, columns), F32)] * 2,
        cost_estimate=cost(1 << 20, 1 << 19),
        compiler_params=room(2),
        name="merge",
    )(parts3, out12, lse12)

    gathered = lax.all_gather(merged, "tp", axis=0, tiled=False)
    gathered = jnp.swapaxes(gathered, 0, 1).reshape(length, -1)
    mixed = jnp.dot(gathered, out_weight, preferred_element_type=F32)
    return mixed.astype(BF)


def solution(mesh):
    weights = P(None, None, "tp")

    def body(*args):
        return per_device(mesh.shape["sp"], *args)

    return jax.shard_map(
        body,
        mesh=mesh,
        in_specs=(P("sp", None), weights, weights, weights, P(None, "tp")),
        out_specs=P("sp", "tp"),
        check_vma=False,
    )
```

```python
import functools

import jax
import jax.numpy as jnp
import numpy as np
from jax import lax
from jax.experimental import pallas as pl
from jax.experimental.pallas import tpu as pltpu
from jax.sharding import PartitionSpec as P


HEAD_DIM = 64
SIDE = 64
MIDDLE = 4
FAR = 16
LANES = 128
ROW = 8
BF = jnp.bfloat16
F32 = jnp.float32
GRANT = 12
PIECES = 2


def rotary_tables(devices, length):
    lane = np.arange(LANES)
    inverse = 10000.0 ** (-2.0 * (lane % (HEAD_DIM // 2)) / HEAD_DIM)
    sign = np.where(lane % HEAD_DIM < HEAD_DIM // 2, -1.0, 1.0)
    base = np.arange(devices)[:, None] * length * inverse[None]
    step = np.arange(length)[:, None] * inverse[None]
    far = np.concatenate([np.cos(base), np.sin(base), sign * np.cos(base), sign * np.sin(base)], axis=1)
    near = np.stack([np.cos(step), np.sin(step)])
    return far.astype(np.float32), near.astype(np.float32)


def turn_tables(row, near):
    cos_base, sin_base = row[:, :LANES], row[:, LANES : 2 * LANES]
    scos_base, ssin_base = row[:, 2 * LANES : 3 * LANES], row[:, 3 * LANES :]
    cos_step, sin_step = near[0], near[1]
    return cos_base * cos_step - sin_base * sin_step, ssin_base * cos_step + scos_base * sin_step


def swap_halves(x):
    lane = lax.broadcasted_iota(jnp.int32, x.shape, 1)
    half = HEAD_DIM // 2
    return jnp.where(
        lane % HEAD_DIM < half, pltpu.roll(x, LANES - half, 1), pltpu.roll(x, half, 1)
    )


def rotate(x, tables):
    return x * tables[0] + swap_halves(x) * tables[1]


def store_by_class(x, scratch, out, dilation):
    scratch[...] = x
    n = x.shape[0] // dilation
    for c in range(dilation):
        out[pl.ds(c * n, n), :] = scratch[pl.ds(c, n, stride=dilation), :].astype(BF)


class Projector:
    def __init__(self, tok, weights, far, near, tok_buf, buf, row_buf, near_buf, sem):
        self.tok_buf, self.buf, self.row_buf, self.near_buf = tok_buf, buf, row_buf, near_buf
        self.sem, self.used = sem, 0
        width = tok.shape[1] // PIECES
        parts = [pl.ds(p * width, width) for p in range(PIECES)]
        self.tokens, self.first = [], []
        for at in parts:
            self.tokens.append(self.start(tok.at[:, at], tok_buf.at[:, at]))
            self.first.append(
                [
                    self.start(ref.at[g, at, :], buf.at[at, pl.ds(n * LANES, LANES)])
                    for n, (ref, g) in enumerate(weights[:2])
                ]
            )
        self.table_copies = [
            self.start(far.at[pl.ds(lax.axis_index("sp"), 1), :], row_buf),
            self.start(near, near_buf),
        ]
        self.later = [
            self.start(ref.at[g], buf.at[:, pl.ds(n * LANES, LANES)])
            for n, (ref, g) in enumerate(weights[2:], 2)
        ]

    def start(self, source, target):
        copy = pltpu.make_async_copy(source, target, self.sem.at[self.used])
        copy.start()
        self.used += 1
        return copy

    def tables(self):
        for copy in self.table_copies:
            copy.wait()
        return turn_tables(self.row_buf[...], self.near_buf)

    def first_pair(self):
        total = None
        width = self.tok_buf.shape[1] // PIECES
        for p in range(PIECES):
            self.tokens[p].wait()
            for copy in self.first[p]:
                copy.wait()
            at = pl.ds(p * width, width)
            part = jnp.dot(
                self.tok_buf[:, at], self.buf[at, : 2 * LANES], preferred_element_type=F32
            )
            total = part if total is None else total + part
        return total

    def product(self, n, count):
        for m in range(count):
            self.later[n - 2 + m].wait()
        return jnp.dot(
            self.tok_buf[...], self.buf[:, pl.ds(n * LANES, count * LANES)],
            preferred_element_type=F32,
        )


def projector_scratch(length, width, weights):
    return [
        pltpu.VMEM((length, width), BF),
        pltpu.VMEM((width, weights * LANES), BF),
        pltpu.VMEM((1, 4 * LANES), F32),
        pltpu.VMEM((2, length, LANES), F32),
        pltpu.SemaphoreType.DMA((3 * PIECES + weights,)),
    ]


def far_kernel(tok, wk, wv, far, near, out, scratch, *buffers):
    work = Projector(tok, ((wk, 2), (wv, 2)), far, near, *buffers)
    both = work.first_pair()
    store_by_class(both[:, LANES:], scratch.at[1], out.at[1], FAR)
    store_by_class(rotate(both[:, :LANES], work.tables()), scratch.at[0], out.at[0], FAR)


def edges_kernel(tok, wq, wk, wv, far, near, q3, kv1, up, down, scratch, *buffers):
    length = tok.shape[0]
    weights = ((wk, 1), (wv, 1), (wk, 0), (wv, 0), (wq, 2))
    work = Projector(tok, weights, far, near, *buffers)
    both = work.first_pair()
    tables = work.tables()
    rows = length // MIDDLE
    for n, x2 in enumerate((rotate(both[:, :LANES], tables), both[:, LANES:])):
        scratch[n] = x2
        for c in range(MIDDLE):
            part = scratch[n, pl.ds(c, rows, stride=MIDDLE), :].astype(BF)
            up[n, pl.ds(c * rows, rows), :] = part
            down[n, pl.ds(c * rows, rows), :] = part
    both = work.product(2, 2)
    for n, x1 in enumerate((rotate(both[:, :LANES], tables), both[:, LANES:])):
        x1 = x1.astype(BF)
        kv1[n] = x1
        up[n, pl.ds(length, SIDE), :] = x1[length - SIDE :]
        down[n, pl.ds(length, SIDE), :] = x1[:SIDE]
    store_by_class(rotate(work.product(4, 1), tables), scratch.at[2], q3, FAR)


def pack_kernel(q3, kv3, halo3, packed):
    size = packed.shape[1] // 5
    for y in range(ROW):
        at = pl.ds(y * size, size)
        for n, part in enumerate((q3[at, :], kv3[0, at, :], kv3[1, at, :], halo3[0, at, :], halo3[1, at, :])):
            packed[y, pl.ds(n * size, size), :] = part


def attend(q, k, v, low, high):
    n, keys = q.shape[0], k.shape[0]
    lane = lax.broadcasted_iota(jnp.int32, (1, LANES), 1)
    first = (lane < HEAD_DIM).astype(F32).astype(BF)
    second = (lane >= HEAD_DIM).astype(F32).astype(BF)
    both = jnp.concatenate([q * first, q * second], axis=0)
    scores = lax.dot_general(both, k, (((1,), (1,)), ((), ())), preferred_element_type=F32)
    scores = scores * HEAD_DIM ** (-0.5)
    column = lax.broadcasted_iota(jnp.int32, (n, keys), 1)
    relative = column - lax.broadcasted_iota(jnp.int32, (n, keys), 0)
    allowed = (relative >= 0) & (relative <= 2 * SIDE) & (column >= low) & (column < high)
    outs, tops, sums = [], [], []
    for head in range(2):
        part = jnp.where(allowed, scores[head * n : (head + 1) * n], -1e30)
        top = jnp.max(part, axis=-1, keepdims=True)
        expo = jnp.exp(part - top)
        sums.append(jnp.sum(expo, axis=-1, keepdims=True))
        tops.append(top)
        outs.append(jnp.dot(expo.astype(BF), v, preferred_element_type=F32))
    is_first = lax.broadcasted_iota(jnp.int32, (n, LANES), 1) < HEAD_DIM
    denom = jnp.where(is_first, sums[0], sums[1])
    top = jnp.where(is_first, tops[0], tops[1])
    return jnp.where(is_first, outs[0], outs[1]) / denom, top + jnp.log(denom)


def merge(out_a, lse_a, out_b, lse_b):
    top = jnp.maximum(lse_a, lse_b)
    wa, wb = jnp.exp(lse_a - top), jnp.exp(lse_b - top)
    total = wa + wb
    return (wa * out_a + wb * out_b) / total, top + jnp.log(total)


def near_attention_kernel(
    devices, tok, wq, far, near, kv1, up, low, high, out, lse, out2, lse2, q12, scratch, *buffers
):
    length = kv1.shape[1]
    work = Projector(tok, ((wq, 0), (wq, 1)), far, near, *buffers)
    both = work.first_pair()
    tables = work.tables()
    q12[0] = rotate(both[:, :LANES], tables).astype(BF)
    store_by_class(rotate(both[:, LANES:], tables), scratch, q12.at[1], MIDDLE)
    me = lax.axis_index("sp")
    rows = length // MIDDLE
    start = jnp.where(me == 0, SIDE, 0)
    for c in range(MIDDLE):
        at = pl.ds(c * rows, rows)
        k = jnp.concatenate([low[0, at, :], up[0, at, :], high[0, at, :]], axis=0)
        v = jnp.concatenate([low[1, at, :], up[1, at, :], high[1, at, :]], axis=0)
        o, l = attend(
            q12[1, at, :], k, v, start, jnp.where(me == devices - 1, 2 * rows, 3 * rows)
        )
        out2[pl.ds(c, rows, stride=MIDDLE), :] = o
        lse2[pl.ds(c, rows, stride=MIDDLE), :] = l
    block = 2 * SIDE
    for b in range(length // block):
        ks, vs = [], []
        for n, xs in enumerate((ks, vs)):
            if b == 0:
                xs.append(low[n, pl.ds(length, SIDE), :])
            first = max(b * block - SIDE, 0)
            last = min((b + 1) * block + SIDE, length)
            xs.append(kv1[n, pl.ds(first, last - first), :])
            if b == length // block - 1:
                xs.append(high[n, pl.ds(length, SIDE), :])
        at = pl.ds(b * block, block)
        o, l = attend(
            q12[0, at, :],
            jnp.concatenate(ks, axis=0),
            jnp.concatenate(vs, axis=0),
            start if b == 0 else 0,
            jnp.where(me == devices - 1, block + SIDE, 2 * block)
            if b == length // block - 1
            else 2 * block,
        )
        out[at, :], lse[at, :] = merge(o, l, out2[at, :], lse2[at, :])


def far_attention_kernel(rows_of_devices, parts, out):
    z = lax.axis_index("sp") // ROW
    low = jnp.where(z == 0, SIDE, 0)
    size = parts.shape[1] // 5
    run = size // 2
    half = ROW // 2
    queries = ROW * run
    high = jnp.where(z == rows_of_devices - 1, queries + SIDE, queries + 2 * SIDE)
    lane = lax.broadcasted_iota(jnp.int32, (queries, LANES), 1)
    for e in range(2):
        piece = lambda a, y: parts[y, pl.ds(a * size + e * run, run), :]
        q = jnp.concatenate([piece(0, y) for y in range(ROW)], axis=0)
        kv = [
            jnp.concatenate(
                [piece(a + 2, y) for y in range(half, ROW)]
                + [piece(a, y) for y in range(ROW)]
                + [piece(a + 2, y) for y in range(half)],
                axis=0,
            )
            for a in (1, 2)
        ]
        o, l = attend(q, kv[0], kv[1], low, high)
        coarse = l.astype(BF).astype(F32)
        l = jnp.where(lane % HEAD_DIM < HEAD_DIM // 2, coarse, l - coarse).astype(BF)
        o = o.astype(BF)
        for y in range(ROW):
            out[y, pl.ds(e * run, run), :] = o[y * run : (y + 1) * run]
            out[y, pl.ds(size + e * run, run), :] = l[y * run : (y + 1) * run]


def merge_kernel(parts, out12, lse12, merged, out3, lse3):
    size = parts.shape[1] // 2
    run = size // 2
    for c in range(FAR):
        y, e = c // 2, c % 2
        at = pl.ds(c, run, stride=FAR)
        out3[at, :] = parts[y, pl.ds(e * run, run), :].astype(F32)
        lse3[at, :] = parts[y, pl.ds(size + e * run, run), :].astype(F32)
    l = lse3[...]
    o, _ = merge(out12[...], lse12[...], out3[...], l + swap_halves(l))
    merged[...] = o.astype(BF)


def output_kernel(gathered, weight, mixed):
    total = None
    columns = gathered.shape[2]
    for n in range(0, gathered.shape[0], 2):
        pair = jnp.concatenate([gathered[n], gathered[n + 1]], axis=1)
        part = jnp.dot(
            pair, weight[pl.ds(n * columns, 2 * columns), :], preferred_element_type=F32
        )
        total = part if total is None else total + part
    mixed[...] = total.astype(BF)


def vmem(shape):
    return jax.ShapeDtypeStruct(shape, BF)


def whole():
    return pl.BlockSpec(memory_space=pltpu.VMEM)


def room(mib):
    return pltpu.CompilerParams(vmem_limit_bytes=int(mib * 1024) << 10)


def cost(flops, size):
    return pl.CostEstimate(flops=flops, bytes_accessed=size, transcendentals=0)


def per_device(devices, tokens, query_weight, key_weight, value_weight, out_weight):
    length, width = tokens.shape
    columns = key_weight.shape[2]
    far, near = rotary_tables(devices, length)
    stay = functools.partial(pltpu.with_memory_space_constraint, memory_space=pltpu.HBM)
    tokens, query_weight, key_weight, value_weight, far, near = (
        stay(x) for x in (tokens, query_weight, key_weight, value_weight, jnp.asarray(far), jnp.asarray(near))
    )
    hbm = pl.BlockSpec(memory_space=pltpu.HBM)
    flat = jax.ShapeDtypeStruct((length, columns), F32)
    scratch = pltpu.VMEM((length, columns), F32)
    kv3 = pl.pallas_call(
        far_kernel,
        in_specs=[hbm] * 5,
        out_specs=whole(),
        out_shape=vmem((2, length, columns)),
        scratch_shapes=[pltpu.VMEM((2, length, columns), F32)]
        + projector_scratch(length, width, 2),
        cost_estimate=cost(4 * length * width * columns, 2 << 20),
        compiler_params=room(GRANT),
        name="far_keys_values",
    )(tokens, key_weight, value_weight, far, near)

    half = ROW // 2
    route = []
    for s in range(devices):
        target = s + ROW if s % ROW >= half else s - ROW
        if 0 <= target < devices:
            route.append((s, target))
    halo3 = lax.ppermute(kv3, "sp", route)

    edge = length + SIDE
    shapes = [
        (length, columns),
        (2, length, columns),
        (2, edge, columns),
        (2, edge, columns),
    ]
    q3, kv1, up, down = pl.pallas_call(
        edges_kernel,
        in_specs=[hbm] * 6,
        out_specs=[whole()] * len(shapes),
        out_shape=[vmem(s) for s in shapes],
        scratch_shapes=[pltpu.VMEM((3, length, columns), F32)]
        + projector_scratch(length, width, 5),
        cost_estimate=cost(10 * length * width * columns, 4 << 20),
        compiler_params=room(GRANT),
        name="projections",
    )(tokens, query_weight, key_weight, value_weight, far, near)

    low = lax.ppermute(up, "sp", [(s, s + 1) for s in range(devices - 1)])
    high = lax.ppermute(down, "sp", [(s + 1, s) for s in range(devices - 1)])

    size = length // ROW
    packed = pl.pallas_call(
        pack_kernel,
        in_specs=[whole()] * 3,
        out_specs=whole(),
        out_shape=vmem((ROW, 5 * size, columns)),
        cost_estimate=cost(1 << 20, 1 << 19),
        compiler_params=room(2),
        name="pack",
    )(q3, kv3, halo3)
    groups = [[z * ROW + y for y in range(ROW)] for z in range(devices // ROW)]
    parts = lax.all_to_all(packed, "sp", 0, 0, axis_index_groups=groups, tiled=True)

    back = pl.pallas_call(
        functools.partial(far_attention_kernel, devices // ROW),
        in_specs=[whole()],
        out_specs=whole(),
        out_shape=vmem((ROW, 2 * size, columns)),
        cost_estimate=cost(1 << 27, 1 << 19),
        compiler_params=room(4),
        name="far_attention",
    )(parts)
    parts3 = lax.all_to_all(back, "sp", 0, 0, axis_index_groups=groups, tiled=True)

    out12, lse12 = pl.pallas_call(
        functools.partial(near_attention_kernel, devices),
        in_specs=[hbm] * 4 + [whole()] * 4,
        out_specs=[whole()] * 2,
        out_shape=[flat, flat],
        scratch_shapes=[scratch, scratch, pltpu.VMEM((2, length, columns), BF), scratch]
        + projector_scratch(length, width, 2),
        cost_estimate=cost(1 << 28, 1 << 20),
        compiler_params=room(GRANT),
        name="near_attention",
    )(tokens, query_weight, far, near, kv1, up, low, high)

    merged = pl.pallas_call(
        merge_kernel,
        in_specs=[whole()] * 3,
        out_specs=whole(),
        out_shape=vmem((length, columns)),
        scratch_shapes=[scratch, scratch],
        cost_estimate=cost(1 << 20, 1 << 19),
        compiler_params=room(2),
        name="merge",
    )(parts3, out12, lse12)

    gathered = lax.all_gather(merged, "tp", axis=0, tiled=False)
    return pl.pallas_call(
        output_kernel,
        in_specs=[whole()] * 2,
        out_specs=whole(),
        out_shape=vmem((length, out_weight.shape[1])),
        cost_estimate=cost(1 << 27, 1 << 20),
        compiler_params=room(4),
        name="output",
    )(gathered, out_weight)


def solution(mesh):
    weights = P(None, None, "tp")

    def body(*args):
        return per_device(mesh.shape["sp"], *args)

    return jax.shard_map(
        body,
        mesh=mesh,
        in_specs=(P("sp", None), weights, weights, weights, P(None, "tp")),
        out_specs=P("sp", "tp"),
        check_vma=False,
    )
```

```python
import functools

import jax
import jax.numpy as jnp
import numpy as np
from jax import lax
from jax.experimental import pallas as pl
from jax.experimental.pallas import tpu as pltpu
from jax.sharding import PartitionSpec as P


HEAD_DIM = 64
SIDE = 64
MIDDLE = 4
FAR = 16
LANES = 128
ROW = 8
BF = jnp.bfloat16
F32 = jnp.float32
GRANT = 12
PIECES = 2


def rotary_tables(devices, length):
    lane = np.arange(LANES)
    inverse = 10000.0 ** (-2.0 * (lane % (HEAD_DIM // 2)) / HEAD_DIM)
    sign = np.where(lane % HEAD_DIM < HEAD_DIM // 2, -1.0, 1.0)
    base = np.arange(devices)[:, None] * length * inverse[None]
    step = np.arange(length)[:, None] * inverse[None]
    far = np.concatenate([np.cos(base), np.sin(base), sign * np.cos(base), sign * np.sin(base)], axis=1)
    near = np.stack([np.cos(step), np.sin(step)])
    return far.astype(np.float32), near.astype(np.float32)


def turn_tables(row, near):
    cos_base, sin_base = row[:, :LANES], row[:, LANES : 2 * LANES]
    scos_base, ssin_base = row[:, 2 * LANES : 3 * LANES], row[:, 3 * LANES :]
    cos_step, sin_step = near[0], near[1]
    return cos_base * cos_step - sin_base * sin_step, ssin_base * cos_step + scos_base * sin_step


def swap_halves(x):
    lane = lax.broadcasted_iota(jnp.int32, x.shape, 1)
    half = HEAD_DIM // 2
    return jnp.where(
        lane % HEAD_DIM < half, pltpu.roll(x, LANES - half, 1), pltpu.roll(x, half, 1)
    )


def rotate(x, tables):
    return x * tables[0] + swap_halves(x) * tables[1]


def store_by_class(x, scratch, out, dilation):
    scratch[...] = x
    n = x.shape[0] // dilation
    for c in range(dilation):
        out[pl.ds(c * n, n), :] = scratch[pl.ds(c, n, stride=dilation), :].astype(BF)


class Projector:
    def __init__(self, tok, weights, far, near, tok_buf, buf, row_buf, near_buf, sem):
        self.tok_buf, self.buf, self.row_buf, self.near_buf = tok_buf, buf, row_buf, near_buf
        self.sem, self.used = sem, 0
        width = tok.shape[1] // PIECES
        parts = [pl.ds(p * width, width) for p in range(PIECES)]
        self.tokens, self.first = [], []
        for at in parts:
            self.tokens.append(self.start(tok.at[:, at], tok_buf.at[:, at]))
            self.first.append(
                [
                    self.start(ref.at[g, at, :], buf.at[at, pl.ds(n * LANES, LANES)])
                    for n, (ref, g) in enumerate(weights[:2])
                ]
            )
        self.table_copies = [
            self.start(far.at[pl.ds(lax.axis_index("sp"), 1), :], row_buf),
            self.start(near, near_buf),
        ]
        self.later = [
            self.start(ref.at[g], buf.at[:, pl.ds(n * LANES, LANES)])
            for n, (ref, g) in enumerate(weights[2:], 2)
        ]

    def start(self, source, target):
        copy = pltpu.make_async_copy(source, target, self.sem.at[self.used])
        copy.start()
        self.used += 1
        return copy

    def tables(self):
        for copy in self.table_copies:
            copy.wait()
        return turn_tables(self.row_buf[...], self.near_buf)

    def first_pair(self):
        total = None
        width = self.tok_buf.shape[1] // PIECES
        for p in range(PIECES):
            self.tokens[p].wait()
            for copy in self.first[p]:
                copy.wait()
            at = pl.ds(p * width, width)
            part = jnp.dot(
                self.tok_buf[:, at], self.buf[at, : 2 * LANES], preferred_element_type=F32
            )
            total = part if total is None else total + part
        return total

    def product(self, n, count):
        for m in range(count):
            self.later[n - 2 + m].wait()
        return jnp.dot(
            self.tok_buf[...], self.buf[:, pl.ds(n * LANES, count * LANES)],
            preferred_element_type=F32,
        )


def projector_scratch(length, width, weights):
    return [
        pltpu.VMEM((length, width), BF),
        pltpu.VMEM((width, weights * LANES), BF),
        pltpu.VMEM((1, 4 * LANES), F32),
        pltpu.VMEM((2, length, LANES), F32),
        pltpu.SemaphoreType.DMA((3 * PIECES + weights,)),
    ]


def far_kernel(tok, wk, wv, far, near, out, scratch, *buffers):
    work = Projector(tok, ((wk, 2), (wv, 2)), far, near, *buffers)
    both = work.first_pair()
    store_by_class(both[:, LANES:], scratch.at[1], out.at[1], FAR)
    store_by_class(rotate(both[:, :LANES], work.tables()), scratch.at[0], out.at[0], FAR)


def edges_kernel(tok, wq, wk, wv, far, near, q3, kv1, up, down, scratch, *buffers):
    length = tok.shape[0]
    weights = ((wk, 1), (wv, 1), (wk, 0), (wv, 0), (wq, 2))
    work = Projector(tok, weights, far, near, *buffers)
    both = work.first_pair()
    tables = work.tables()
    rows = length // MIDDLE
    for n, x2 in enumerate((rotate(both[:, :LANES], tables), both[:, LANES:])):
        scratch[n] = x2
        for c in range(MIDDLE):
            part = scratch[n, pl.ds(c, rows, stride=MIDDLE), :].astype(BF)
            up[n, pl.ds(c * rows, rows), :] = part
            down[n, pl.ds(c * rows, rows), :] = part
    both = work.product(2, 2)
    for n, x1 in enumerate((rotate(both[:, :LANES], tables), both[:, LANES:])):
        x1 = x1.astype(BF)
        kv1[n] = x1
        up[n, pl.ds(length, SIDE), :] = x1[length - SIDE :]
        down[n, pl.ds(length, SIDE), :] = x1[:SIDE]
    store_by_class(rotate(work.product(4, 1), tables), scratch.at[2], q3, FAR)


def pack_kernel(q3, kv3, halo3, packed):
    size = packed.shape[1] // 5
    for y in range(ROW):
        at = pl.ds(y * size, size)
        for n, part in enumerate((q3[at, :], kv3[0, at, :], kv3[1, at, :], halo3[0, at, :], halo3[1, at, :])):
            packed[y, pl.ds(n * size, size), :] = part


def attend(q, k, v, low, high):
    n, keys = q.shape[0], k.shape[0]
    lane = lax.broadcasted_iota(jnp.int32, (1, LANES), 1)
    first = (lane < HEAD_DIM).astype(F32).astype(BF)
    second = (lane >= HEAD_DIM).astype(F32).astype(BF)
    both = jnp.concatenate([q * first, q * second], axis=0)
    scores = lax.dot_general(both, k, (((1,), (1,)), ((), ())), preferred_element_type=F32)
    scores = scores * HEAD_DIM ** (-0.5)
    column = lax.broadcasted_iota(jnp.int32, (n, keys), 1)
    relative = column - lax.broadcasted_iota(jnp.int32, (n, keys), 0)
    allowed = (relative >= 0) & (relative <= 2 * SIDE) & (column >= low) & (column < high)
    outs, tops, sums = [], [], []
    for head in range(2):
        part = jnp.where(allowed, scores[head * n : (head + 1) * n], -1e30)
        top = jnp.max(part, axis=-1, keepdims=True)
        expo = jnp.exp(part - top)
        sums.append(jnp.sum(expo, axis=-1, keepdims=True))
        tops.append(top)
        outs.append(jnp.dot(expo.astype(BF), v, preferred_element_type=F32))
    is_first = lax.broadcasted_iota(jnp.int32, (n, LANES), 1) < HEAD_DIM
    denom = jnp.where(is_first, sums[0], sums[1])
    top = jnp.where(is_first, tops[0], tops[1])
    return jnp.where(is_first, outs[0], outs[1]) / denom, top + jnp.log(denom)


def merge(out_a, lse_a, out_b, lse_b):
    top = jnp.maximum(lse_a, lse_b)
    wa, wb = jnp.exp(lse_a - top), jnp.exp(lse_b - top)
    total = wa + wb
    return (wa * out_a + wb * out_b) / total, top + jnp.log(total)


def near_attention_kernel(
    devices, tok, wq, far, near, kv1, up, low, high, out, lse, out2, lse2, q12, scratch, *buffers
):
    length = kv1.shape[1]
    work = Projector(tok, ((wq, 0), (wq, 1)), far, near, *buffers)
    both = work.first_pair()
    tables = work.tables()
    q12[0] = rotate(both[:, :LANES], tables).astype(BF)
    store_by_class(rotate(both[:, LANES:], tables), scratch, q12.at[1], MIDDLE)
    me = lax.axis_index("sp")
    rows = length // MIDDLE
    start = jnp.where(me == 0, SIDE, 0)
    for c in range(MIDDLE):
        at = pl.ds(c * rows, rows)
        k = jnp.concatenate([low[0, at, :], up[0, at, :], high[0, at, :]], axis=0)
        v = jnp.concatenate([low[1, at, :], up[1, at, :], high[1, at, :]], axis=0)
        o, l = attend(
            q12[1, at, :], k, v, start, jnp.where(me == devices - 1, 2 * rows, 3 * rows)
        )
        out2[pl.ds(c, rows, stride=MIDDLE), :] = o
        lse2[pl.ds(c, rows, stride=MIDDLE), :] = l
    block = 2 * SIDE
    for b in range(length // block):
        ks, vs = [], []
        for n, xs in enumerate((ks, vs)):
            if b == 0:
                xs.append(low[n, pl.ds(length, SIDE), :])
            first = max(b * block - SIDE, 0)
            last = min((b + 1) * block + SIDE, length)
            xs.append(kv1[n, pl.ds(first, last - first), :])
            if b == length // block - 1:
                xs.append(high[n, pl.ds(length, SIDE), :])
        at = pl.ds(b * block, block)
        o, l = attend(
            q12[0, at, :],
            jnp.concatenate(ks, axis=0),
            jnp.concatenate(vs, axis=0),
            start if b == 0 else 0,
            jnp.where(me == devices - 1, block + SIDE, 2 * block)
            if b == length // block - 1
            else 2 * block,
        )
        out[at, :], lse[at, :] = merge(o, l, out2[at, :], lse2[at, :])


def far_attention_kernel(rows_of_devices, parts, out):
    z = lax.axis_index("sp") // ROW
    low = jnp.where(z == 0, SIDE, 0)
    size = parts.shape[1] // 5
    run = size // 2
    half = ROW // 2
    queries = ROW * run
    high = jnp.where(z == rows_of_devices - 1, queries + SIDE, queries + 2 * SIDE)
    lane = lax.broadcasted_iota(jnp.int32, (queries, LANES), 1)
    for e in range(2):
        piece = lambda a, y: parts[y, pl.ds(a * size + e * run, run), :]
        q = jnp.concatenate([piece(0, y) for y in range(ROW)], axis=0)
        kv = [
            jnp.concatenate(
                [piece(a + 2, y) for y in range(half, ROW)]
                + [piece(a, y) for y in range(ROW)]
                + [piece(a + 2, y) for y in range(half)],
                axis=0,
            )
            for a in (1, 2)
        ]
        o, l = attend(q, kv[0], kv[1], low, high)
        coarse = l.astype(BF).astype(F32)
        l = jnp.where(lane % HEAD_DIM < HEAD_DIM // 2, coarse, l - coarse).astype(BF)
        o = o.astype(BF)
        for y in range(ROW):
            out[y, pl.ds(e * run, run), :] = o[y * run : (y + 1) * run]
            out[y, pl.ds(size + e * run, run), :] = l[y * run : (y + 1) * run]


def merge_kernel(parts, out12, lse12, merged, out3, lse3):
    size = parts.shape[1] // 2
    run = size // 2
    for c in range(FAR):
        y, e = c // 2, c % 2
        at = pl.ds(c, run, stride=FAR)
        out3[at, :] = parts[y, pl.ds(e * run, run), :].astype(F32)
        lse3[at, :] = parts[y, pl.ds(size + e * run, run), :].astype(F32)
    l = lse3[...]
    o, _ = merge(out12[...], lse12[...], out3[...], l + swap_halves(l))
    o = o.astype(BF)
    for n in range(merged.shape[0]):
        merged[n] = o


def output_kernel(gathered, weight, mixed):
    total = None
    columns = gathered.shape[3]
    for n in range(gathered.shape[1]):
        pair = jnp.concatenate([gathered[0, n], gathered[1, n]], axis=1)
        part = jnp.dot(
            pair, weight[pl.ds(2 * n * columns, 2 * columns), :], preferred_element_type=F32
        )
        total = part if total is None else total + part
    mixed[...] = total.astype(BF)


def vmem(shape):
    return jax.ShapeDtypeStruct(shape, BF)


def whole():
    return pl.BlockSpec(memory_space=pltpu.VMEM)


def room(mib):
    return pltpu.CompilerParams(vmem_limit_bytes=int(mib * 1024) << 10)


def cost(flops, size):
    return pl.CostEstimate(flops=flops, bytes_accessed=size, transcendentals=0)


def per_device(devices, tokens, query_weight, key_weight, value_weight, out_weight):
    length, width = tokens.shape
    columns = key_weight.shape[2]
    far, near = rotary_tables(devices, length)
    stay = functools.partial(pltpu.with_memory_space_constraint, memory_space=pltpu.HBM)
    tokens, query_weight, key_weight, value_weight, far, near = (
        stay(x) for x in (tokens, query_weight, key_weight, value_weight, jnp.asarray(far), jnp.asarray(near))
    )
    hbm = pl.BlockSpec(memory_space=pltpu.HBM)
    flat = jax.ShapeDtypeStruct((length, columns), F32)
    scratch = pltpu.VMEM((length, columns), F32)
    kv3 = pl.pallas_call(
        far_kernel,
        in_specs=[hbm] * 5,
        out_specs=whole(),
        out_shape=vmem((2, length, columns)),
        scratch_shapes=[pltpu.VMEM((2, length, columns), F32)]
        + projector_scratch(length, width, 2),
        cost_estimate=cost(4 * length * width * columns, 2 << 20),
        compiler_params=room(GRANT),
        name="far_keys_values",
    )(tokens, key_weight, value_weight, far, near)

    half = ROW // 2
    route = []
    for s in range(devices):
        target = s + ROW if s % ROW >= half else s - ROW
        if 0 <= target < devices:
            route.append((s, target))
    halo3 = lax.ppermute(kv3, "sp", route)

    edge = length + SIDE
    shapes = [
        (length, columns),
        (2, length, columns),
        (2, edge, columns),
        (2, edge, columns),
    ]
    q3, kv1, up, down = pl.pallas_call(
        edges_kernel,
        in_specs=[hbm] * 6,
        out_specs=[whole()] * len(shapes),
        out_shape=[vmem(s) for s in shapes],
        scratch_shapes=[pltpu.VMEM((3, length, columns), F32)]
        + projector_scratch(length, width, 5),
        cost_estimate=cost(10 * length * width * columns, 4 << 20),
        compiler_params=room(GRANT),
        name="projections",
    )(tokens, query_weight, key_weight, value_weight, far, near)

    low = lax.ppermute(up, "sp", [(s, s + 1) for s in range(devices - 1)])
    high = lax.ppermute(down, "sp", [(s + 1, s) for s in range(devices - 1)])

    size = length // ROW
    packed = pl.pallas_call(
        pack_kernel,
        in_specs=[whole()] * 3,
        out_specs=whole(),
        out_shape=vmem((ROW, 5 * size, columns)),
        cost_estimate=cost(1 << 20, 1 << 19),
        compiler_params=room(2),
        name="pack",
    )(q3, kv3, halo3)
    groups = [[z * ROW + y for y in range(ROW)] for z in range(devices // ROW)]
    parts = lax.all_to_all(packed, "sp", 0, 0, axis_index_groups=groups, tiled=True)

    back = pl.pallas_call(
        functools.partial(far_attention_kernel, devices // ROW),
        in_specs=[whole()],
        out_specs=whole(),
        out_shape=vmem((ROW, 2 * size, columns)),
        cost_estimate=cost(1 << 27, 1 << 19),
        compiler_params=room(4),
        name="far_attention",
    )(parts)
    parts3 = lax.all_to_all(back, "sp", 0, 0, axis_index_groups=groups, tiled=True)

    out12, lse12 = pl.pallas_call(
        functools.partial(near_attention_kernel, devices),
        in_specs=[hbm] * 4 + [whole()] * 4,
        out_specs=[whole()] * 2,
        out_shape=[flat, flat],
        scratch_shapes=[scratch, scratch, pltpu.VMEM((2, length, columns), BF), scratch]
        + projector_scratch(length, width, 2),
        cost_estimate=cost(1 << 28, 1 << 20),
        compiler_params=room(GRANT),
        name="near_attention",
    )(tokens, query_weight, far, near, kv1, up, low, high)

    chips = lax.axis_size("tp") // 2
    merged = pl.pallas_call(
        merge_kernel,
        in_specs=[whole()] * 3,
        out_specs=whole(),
        out_shape=vmem((chips, length, columns)),
        scratch_shapes=[scratch, scratch],
        cost_estimate=cost(1 << 20, 1 << 19),
        compiler_params=room(2),
        name="merge",
    )(parts3, out12, lse12)

    lines = [[2 * n + core for n in range(chips)] for core in range(2)]
    gathered = lax.all_to_all(merged, "tp", 0, 0, axis_index_groups=lines, tiled=True)
    cores = [[2 * n, 2 * n + 1] for n in range(chips)]
    gathered = lax.all_gather(gathered, "tp", axis=0, axis_index_groups=cores)
    return pl.pallas_call(
        output_kernel,
        in_specs=[whole()] * 2,
        out_specs=whole(),
        out_shape=vmem((length, out_weight.shape[1])),
        cost_estimate=cost(1 << 27, 1 << 20),
        compiler_params=room(4),
        name="output",
    )(gathered, out_weight)


def solution(mesh):
    weights = P(None, None, "tp")

    def body(*args):
        return per_device(mesh.shape["sp"], *args)

    return jax.shard_map(
        body,
        mesh=mesh,
        in_specs=(P("sp", None), weights, weights, weights, P(None, "tp")),
        out_specs=P("sp", "tp"),
        check_vma=False,
    )
```

```python
import functools

import jax
import jax.numpy as jnp
import numpy as np
from jax import lax
from jax.experimental import pallas as pl
from jax.experimental.pallas import tpu as pltpu
from jax.sharding import PartitionSpec as P


HEAD_DIM = 64
SIDE = 64
MIDDLE = 4
FAR = 16
LANES = 128
ROW = 8
BF = jnp.bfloat16
F32 = jnp.float32
ORDER = (0, 4, 1, 5, 2, 6, 3, 7)
SLOT = tuple(ORDER.index(y) for y in range(ROW))
CHIPS = (0, 2, 1, 3)
FOLD = 8
GRANT = 12
PIECES = 2


def rotary_tables(devices, length):
    lane = np.arange(LANES)
    inverse = 10000.0 ** (-2.0 * (lane % (HEAD_DIM // 2)) / HEAD_DIM)
    sign = np.where(lane % HEAD_DIM < HEAD_DIM // 2, -1.0, 1.0)
    base = np.arange(devices)[:, None] * length * inverse[None]
    step = np.arange(length)[:, None] * inverse[None]
    far = np.concatenate([np.cos(base), np.sin(base), sign * np.cos(base), sign * np.sin(base)], axis=1)
    near = np.stack([np.cos(step), np.sin(step)])
    return far.astype(np.float32), near.astype(np.float32)


def turn_tables(row, near):
    cos_base, sin_base = row[:, :LANES], row[:, LANES : 2 * LANES]
    scos_base, ssin_base = row[:, 2 * LANES : 3 * LANES], row[:, 3 * LANES :]
    cos_step, sin_step = near[0], near[1]
    return cos_base * cos_step - sin_base * sin_step, ssin_base * cos_step + scos_base * sin_step


def swap_halves(x):
    lane = lax.broadcasted_iota(jnp.int32, x.shape, 1)
    half = HEAD_DIM // 2
    return jnp.where(
        lane % HEAD_DIM < half, pltpu.roll(x, LANES - half, 1), pltpu.roll(x, half, 1)
    )


def rotate(x, tables):
    return x * tables[0] + swap_halves(x) * tables[1]


def store_by_class(x, scratch, out, dilation):
    scratch[...] = x
    n = x.shape[0] // dilation
    for c in range(dilation):
        out[pl.ds(c * n, n), :] = scratch[pl.ds(c, n, stride=dilation), :].astype(BF)


class Projector:
    def __init__(self, tok, weights, far, near, tok_buf, buf, row_buf, near_buf, sem):
        self.tok_buf, self.buf, self.row_buf, self.near_buf = tok_buf, buf, row_buf, near_buf
        self.sem, self.used = sem, 0
        width = tok.shape[1] // PIECES
        parts = [pl.ds(p * width, width) for p in range(PIECES)]
        self.tokens, self.first = [], []
        for at in parts:
            self.tokens.append(self.start(tok.at[:, at], tok_buf.at[:, at]))
            self.first.append(
                [
                    self.start(ref.at[g, at, :], buf.at[at, pl.ds(n * LANES, LANES)])
                    for n, (ref, g) in enumerate(weights[:2])
                ]
            )
        self.table_copies = [
            self.start(far.at[pl.ds(lax.axis_index("sp"), 1), :], row_buf),
            self.start(near, near_buf),
        ]
        self.later = [
            self.start(ref.at[g], buf.at[:, pl.ds(n * LANES, LANES)])
            for n, (ref, g) in enumerate(weights[2:], 2)
        ]

    def start(self, source, target):
        copy = pltpu.make_async_copy(source, target, self.sem.at[self.used])
        copy.start()
        self.used += 1
        return copy

    def tables(self):
        for copy in self.table_copies:
            copy.wait()
        return turn_tables(self.row_buf[...], self.near_buf)

    def first_pair(self):
        total = None
        width = self.tok_buf.shape[1] // PIECES
        for p in range(PIECES):
            self.tokens[p].wait()
            for copy in self.first[p]:
                copy.wait()
            at = pl.ds(p * width, width)
            part = jnp.dot(
                self.tok_buf[:, at], self.buf[at, : 2 * LANES], preferred_element_type=F32
            )
            total = part if total is None else total + part
        return total

    def product(self, n, count):
        for m in range(count):
            self.later[n - 2 + m].wait()
        return jnp.dot(
            self.tok_buf[...], self.buf[:, pl.ds(n * LANES, count * LANES)],
            preferred_element_type=F32,
        )


def projector_scratch(length, width, weights):
    return [
        pltpu.VMEM((length, width), BF),
        pltpu.VMEM((width, weights * LANES), BF),
        pltpu.VMEM((1, 4 * LANES), F32),
        pltpu.VMEM((2, length, LANES), F32),
        pltpu.SemaphoreType.DMA((3 * PIECES + weights,)),
    ]


def far_kernel(tok, wk, wv, far, near, out, scratch, *buffers):
    work = Projector(tok, ((wk, 2), (wv, 2)), far, near, *buffers)
    both = work.first_pair()
    store_by_class(both[:, LANES:], scratch.at[1], out.at[1], FAR)
    store_by_class(rotate(both[:, :LANES], work.tables()), scratch.at[0], out.at[0], FAR)


def edges_kernel(tok, wq, wk, wv, far, near, q3, kv1, up, down, scratch, *buffers):
    length = tok.shape[0]
    weights = ((wk, 1), (wv, 1), (wk, 0), (wv, 0), (wq, 2))
    work = Projector(tok, weights, far, near, *buffers)
    both = work.first_pair()
    tables = work.tables()
    rows = length // MIDDLE
    for n, x2 in enumerate((rotate(both[:, :LANES], tables), both[:, LANES:])):
        scratch[n] = x2
        for c in range(MIDDLE):
            part = scratch[n, pl.ds(c, rows, stride=MIDDLE), :].astype(BF)
            up[n, pl.ds(c * rows, rows), :] = part
            down[n, pl.ds(c * rows, rows), :] = part
    both = work.product(2, 2)
    for n, x1 in enumerate((rotate(both[:, :LANES], tables), both[:, LANES:])):
        x1 = x1.astype(BF)
        kv1[n] = x1
        up[n, pl.ds(length, SIDE), :] = x1[length - SIDE :]
        down[n, pl.ds(length, SIDE), :] = x1[:SIDE]
    store_by_class(rotate(work.product(4, 1), tables), scratch.at[2], q3, FAR)


def pack_kernel(q3, kv3, halo3, packed, sem):
    size = packed.shape[1] // 5
    copies = []
    for n, part in enumerate((q3, kv3.at[0], kv3.at[1], halo3.at[0], halo3.at[1])):
        for y in range(ROW):
            copy = pltpu.make_async_copy(
                part.at[pl.ds(y * size, size), :],
                packed.at[SLOT[y], pl.ds(n * size, size), :],
                sem.at[n * ROW + y],
            )
            copy.start()
            copies.append(copy)
    for copy in copies:
        copy.wait()


def attend(q, k, v, low, high):
    n, keys = q.shape[0], k.shape[0]
    lane = lax.broadcasted_iota(jnp.int32, (1, LANES), 1)
    first = (lane < HEAD_DIM).astype(F32).astype(BF)
    second = (lane >= HEAD_DIM).astype(F32).astype(BF)
    both = jnp.concatenate([q * first, q * second], axis=0)
    scores = lax.dot_general(both, k, (((1,), (1,)), ((), ())), preferred_element_type=F32)
    scores = scores * HEAD_DIM ** (-0.5)
    column = lax.broadcasted_iota(jnp.int32, (n, keys), 1)
    relative = column - lax.broadcasted_iota(jnp.int32, (n, keys), 0)
    allowed = (relative >= 0) & (relative <= 2 * SIDE) & (column >= low) & (column < high)
    outs, tops, sums = [], [], []
    for head in range(2):
        part = jnp.where(allowed, scores[head * n : (head + 1) * n], -1e30)
        top = jnp.max(part, axis=-1, keepdims=True)
        expo = jnp.exp(part - top)
        sums.append(jnp.sum(expo, axis=-1, keepdims=True))
        tops.append(top)
        outs.append(jnp.dot(expo.astype(BF), v, preferred_element_type=F32))
    is_first = lax.broadcasted_iota(jnp.int32, (n, LANES), 1) < HEAD_DIM
    denom = jnp.where(is_first, sums[0], sums[1])
    lse = [t + jnp.log(d) for t, d in zip(tops, sums)]
    return jnp.where(is_first, outs[0], outs[1]) / denom, lse


def spread(lse, rows):
    return jnp.where(lax.broadcasted_iota(jnp.int32, (rows, LANES), 1) < HEAD_DIM, lse[0], lse[1])


def merge(out_a, lse_a, out_b, lse_b):
    top = jnp.maximum(lse_a, lse_b)
    wa, wb = jnp.exp(lse_a - top), jnp.exp(lse_b - top)
    total = wa + wb
    return (wa * out_a + wb * out_b) / total, top + jnp.log(total)


def near_attention_kernel(
    devices, tok, wq, far, near, kv1, up, low, high, out, lse, out2, lse2, q12, scratch, *buffers
):
    length = kv1.shape[1]
    work = Projector(tok, ((wq, 0), (wq, 1)), far, near, *buffers)
    both = work.first_pair()
    tables = work.tables()
    q12[0] = rotate(both[:, :LANES], tables).astype(BF)
    store_by_class(rotate(both[:, LANES:], tables), scratch, q12.at[1], MIDDLE)
    me = lax.axis_index("sp")
    rows = length // MIDDLE
    start = jnp.where(me == 0, SIDE, 0)
    for c in range(MIDDLE):
        at = pl.ds(c * rows, rows)
        k = jnp.concatenate([low[0, at, :], up[0, at, :], high[0, at, :]], axis=0)
        v = jnp.concatenate([low[1, at, :], up[1, at, :], high[1, at, :]], axis=0)
        o, l = attend(
            q12[1, at, :], k, v, start, jnp.where(me == devices - 1, 2 * rows, 3 * rows)
        )
        out2[pl.ds(c, rows, stride=MIDDLE), :] = o
        lse2[pl.ds(c, rows, stride=MIDDLE), :] = spread(l, rows)
    block = 2 * SIDE
    for b in range(length // block):
        ks, vs = [], []
        for n, xs in enumerate((ks, vs)):
            if b == 0:
                xs.append(low[n, pl.ds(length, SIDE), :])
            first = max(b * block - SIDE, 0)
            last = min((b + 1) * block + SIDE, length)
            xs.append(kv1[n, pl.ds(first, last - first), :])
            if b == length // block - 1:
                xs.append(high[n, pl.ds(length, SIDE), :])
        at = pl.ds(b * block, block)
        o, l = attend(
            q12[0, at, :],
            jnp.concatenate(ks, axis=0),
            jnp.concatenate(vs, axis=0),
            start if b == 0 else 0,
            jnp.where(me == devices - 1, block + SIDE, 2 * block)
            if b == length // block - 1
            else 2 * block,
        )
        out[at, :], lse[at, :] = merge(
            o, spread(l, block), out2[at, :], lse2[at, :]
        )


def far_attention_kernel(rows_of_devices, parts, out):
    z = lax.axis_index("sp") // ROW
    low = jnp.where(z == 0, SIDE, 0)
    size = parts.shape[1] // 5
    run = size // 2
    half = ROW // 2
    queries = ROW * run
    high = jnp.where(z == rows_of_devices - 1, queries + SIDE, queries + 2 * SIDE)
    lane = lax.broadcasted_iota(jnp.int32, (queries, LANES), 1)
    group = lax.broadcasted_iota(jnp.int32, (FOLD, LANES), 1) // (LANES // 4)
    which = lane // (LANES // 16) % 4
    folded = [jnp.zeros((FOLD, LANES), F32) for _ in range(ROW)]
    for e in range(2):
        piece = lambda a, y: parts[SLOT[y], pl.ds(a * size + e * run, run), :]
        q = jnp.concatenate([piece(0, y) for y in range(ROW)], axis=0)
        kv = [
            jnp.concatenate(
                [piece(a + 2, y) for y in range(half, ROW)]
                + [piece(a, y) for y in range(ROW)]
                + [piece(a + 2, y) for y in range(half)],
                axis=0,
            )
            for a in (1, 2)
        ]
        o, l = attend(q, kv[0], kv[1], low, high)
        coarse = [x.astype(BF).astype(F32) for x in l]
        fine = [x - c for x, c in zip(l, coarse)]
        terms = jnp.where(
            which < 2,
            jnp.where(which == 0, coarse[0], fine[0]),
            jnp.where(which == 2, coarse[1], fine[1]),
        )
        o = o.astype(BF)
        for y in range(ROW):
            out[SLOT[y], pl.ds(e * run, run), :] = o[y * run : (y + 1) * run]
            for h in range(2):
                at = y * run + h * FOLD
                folded[y] = jnp.where(group == 2 * e + h, terms[at : at + FOLD], folded[y])
    for y in range(ROW):
        out[SLOT[y], pl.ds(size, FOLD), :] = folded[y].astype(BF)


def merge_kernel(parts, out12, lse12, merged, out3, lse3):
    run = merged.shape[1] // FAR
    size = 2 * run
    quarter, eighth = LANES // 4, LANES // 8
    for y in range(ROW):
        terms = parts[SLOT[y], pl.ds(size, FOLD), :].astype(F32)
        total = terms + pltpu.roll(terms, LANES - LANES // 16, 1)
        for e in range(2):
            at = pl.ds(2 * y + e, run, stride=FAR)
            out3[at, :] = parts[SLOT[y], pl.ds(e * run, run), :].astype(F32)
            rows = []
            for h in range(2):
                n = (2 * e + h) * quarter
                rows.append(spread((total[:, n : n + 1], total[:, n + eighth : n + eighth + 1]), FOLD))
            lse3[at, :] = jnp.concatenate(rows, axis=0)
    o, _ = merge(out12[...], lse12[...], out3[...], lse3[...])
    o = o.astype(BF)
    for n in range(merged.shape[0]):
        merged[n] = o


def output_kernel(gathered, weight, mixed):
    total = None
    columns = gathered.shape[3]
    for at, n in enumerate(CHIPS):
        pair = jnp.concatenate([gathered[0, at], gathered[1, at]], axis=1)
        part = jnp.dot(
            pair, weight[pl.ds(2 * n * columns, 2 * columns), :], preferred_element_type=F32
        )
        total = part if total is None else total + part
    mixed[...] = total.astype(BF)


def vmem(shape):
    return jax.ShapeDtypeStruct(shape, BF)


def whole():
    return pl.BlockSpec(memory_space=pltpu.VMEM)


def room(mib):
    return pltpu.CompilerParams(vmem_limit_bytes=int(mib * 1024) << 10)


def cost(flops, size):
    return pl.CostEstimate(flops=flops, bytes_accessed=size, transcendentals=0)


def per_device(devices, tokens, query_weight, key_weight, value_weight, out_weight):
    length, width = tokens.shape
    columns = key_weight.shape[2]
    far, near = rotary_tables(devices, length)
    stay = functools.partial(pltpu.with_memory_space_constraint, memory_space=pltpu.HBM)
    tokens, query_weight, key_weight, value_weight, far, near = (
        stay(x) for x in (tokens, query_weight, key_weight, value_weight, jnp.asarray(far), jnp.asarray(near))
    )
    hbm = pl.BlockSpec(memory_space=pltpu.HBM)
    flat = jax.ShapeDtypeStruct((length, columns), F32)
    scratch = pltpu.VMEM((length, columns), F32)
    kv3 = pl.pallas_call(
        far_kernel,
        in_specs=[hbm] * 5,
        out_specs=whole(),
        out_shape=vmem((2, length, columns)),
        scratch_shapes=[pltpu.VMEM((2, length, columns), F32)]
        + projector_scratch(length, width, 2),
        cost_estimate=cost(4 * length * width * columns, 2 << 20),
        compiler_params=room(GRANT),
        name="far_keys_values",
    )(tokens, key_weight, value_weight, far, near)

    half = ROW // 2
    route = []
    for s in range(devices):
        target = s + ROW if s % ROW >= half else s - ROW
        if 0 <= target < devices:
            route.append((s, target))
    halo3 = lax.ppermute(kv3, "sp", route)

    edge = length + SIDE
    shapes = [
        (length, columns),
        (2, length, columns),
        (2, edge, columns),
        (2, edge, columns),
    ]
    q3, kv1, up, down = pl.pallas_call(
        edges_kernel,
        in_specs=[hbm] * 6,
        out_specs=[whole()] * len(shapes),
        out_shape=[vmem(s) for s in shapes],
        scratch_shapes=[pltpu.VMEM((3, length, columns), F32)]
        + projector_scratch(length, width, 5),
        cost_estimate=cost(10 * length * width * columns, 4 << 20),
        compiler_params=room(GRANT),
        name="projections",
    )(tokens, query_weight, key_weight, value_weight, far, near)

    low = lax.ppermute(up, "sp", [(s, s + 1) for s in range(devices - 1)])
    high = lax.ppermute(down, "sp", [(s + 1, s) for s in range(devices - 1)])

    size = length // ROW
    packed = pl.pallas_call(
        pack_kernel,
        in_specs=[whole()] * 3,
        out_specs=hbm,
        out_shape=vmem((ROW, 5 * size, columns)),
        scratch_shapes=[pltpu.SemaphoreType.DMA((5 * ROW,))],
        cost_estimate=cost(1 << 20, 1 << 19),
        compiler_params=room(2),
        name="pack",
    )(q3, kv3, halo3)
    groups = [[z * ROW + y for y in ORDER] for z in range(devices // ROW)]
    parts = lax.all_to_all(packed, "sp", 0, 0, axis_index_groups=groups, tiled=True)

    back = pl.pallas_call(
        functools.partial(far_attention_kernel, devices // ROW),
        in_specs=[whole()],
        out_specs=whole(),
        out_shape=vmem((ROW, size + FOLD, columns)),
        cost_estimate=cost(1 << 27, 1 << 19),
        compiler_params=room(4),
        name="far_attention",
    )(parts)
    parts3 = lax.all_to_all(back, "sp", 0, 0, axis_index_groups=groups, tiled=True)

    out12, lse12 = pl.pallas_call(
        functools.partial(near_attention_kernel, devices),
        in_specs=[hbm] * 4 + [whole()] * 4,
        out_specs=[whole()] * 2,
        out_shape=[flat, flat],
        scratch_shapes=[scratch, scratch, pltpu.VMEM((2, length, columns), BF), scratch]
        + projector_scratch(length, width, 2),
        cost_estimate=cost(1 << 28, 1 << 20),
        compiler_params=room(GRANT),
        name="near_attention",
    )(tokens, query_weight, far, near, kv1, up, low, high)

    chips = lax.axis_size("tp") // 2
    merged = pl.pallas_call(
        merge_kernel,
        in_specs=[whole()] * 3,
        out_specs=whole(),
        out_shape=vmem((chips, length, columns)),
        scratch_shapes=[scratch, scratch],
        cost_estimate=cost(1 << 20, 1 << 19),
        compiler_params=room(2),
        name="merge",
    )(parts3, out12, lse12)

    lines = [[2 * n + core for n in CHIPS] for core in range(2)]
    gathered = lax.all_to_all(merged, "tp", 0, 0, axis_index_groups=lines, tiled=True)
    cores = [[2 * n, 2 * n + 1] for n in range(chips)]
    gathered = lax.all_gather(gathered, "tp", axis=0, axis_index_groups=cores)
    return pl.pallas_call(
        output_kernel,
        in_specs=[whole()] * 2,
        out_specs=whole(),
        out_shape=vmem((length, out_weight.shape[1])),
        cost_estimate=cost(1 << 27, 1 << 20),
        compiler_params=room(4),
        name="output",
    )(gathered, out_weight)


def solution(mesh):
    weights = P(None, None, "tp")

    def body(*args):
        return per_device(mesh.shape["sp"], *args)

    return jax.shard_map(
        body,
        mesh=mesh,
        in_specs=(P("sp", None), weights, weights, weights, P(None, "tp")),
        out_specs=P("sp", "tp"),
        check_vma=False,
    )
```

```python
import functools

import jax
import jax.numpy as jnp
import numpy as np
from jax import lax
from jax.experimental import pallas as pl
from jax.experimental.pallas import tpu as pltpu
from jax.sharding import PartitionSpec as P


HEAD_DIM = 64
SIDE = 64
MIDDLE = 4
FAR = 16
LANES = 128
ROW = 8
BF = jnp.bfloat16
F32 = jnp.float32
ORDER = (0, 4, 2, 6, 1, 5, 3, 7)
SLOT = tuple(ORDER.index(y) for y in range(ROW))
CHIPS = (0, 2, 1, 3)
FOLD = 8
GRANT = 12
PIECES = 2


def rotary_tables(devices, length):
    lane = np.arange(LANES)
    inverse = 10000.0 ** (-2.0 * (lane % (HEAD_DIM // 2)) / HEAD_DIM)
    sign = np.where(lane % HEAD_DIM < HEAD_DIM // 2, -1.0, 1.0)
    base = np.arange(devices)[:, None] * length * inverse[None]
    step = np.arange(length)[:, None] * inverse[None]
    far = np.concatenate([np.cos(base), np.sin(base), sign * np.cos(base), sign * np.sin(base)], axis=1)
    near = np.stack([np.cos(step), np.sin(step)])
    return far.astype(np.float32), near.astype(np.float32)


def turn_tables(row, near):
    cos_base, sin_base = row[:, :LANES], row[:, LANES : 2 * LANES]
    scos_base, ssin_base = row[:, 2 * LANES : 3 * LANES], row[:, 3 * LANES :]
    cos_step, sin_step = near[0], near[1]
    return cos_base * cos_step - sin_base * sin_step, ssin_base * cos_step + scos_base * sin_step


def swap_halves(x):
    lane = lax.broadcasted_iota(jnp.int32, x.shape, 1)
    half = HEAD_DIM // 2
    return jnp.where(
        lane % HEAD_DIM < half, pltpu.roll(x, LANES - half, 1), pltpu.roll(x, half, 1)
    )


def rotate(x, tables):
    return x * tables[0] + swap_halves(x) * tables[1]


def store_by_class(x, scratch, out, dilation):
    scratch[...] = x
    n = x.shape[0] // dilation
    for c in range(dilation):
        out[pl.ds(c * n, n), :] = scratch[pl.ds(c, n, stride=dilation), :].astype(BF)


class Projector:
    def __init__(self, tok, weights, far, near, tok_buf, buf, row_buf, near_buf, sem):
        self.tok_buf, self.buf, self.row_buf, self.near_buf = tok_buf, buf, row_buf, near_buf
        self.sem, self.used = sem, 0
        width = tok.shape[1] // PIECES
        parts = [pl.ds(p * width, width) for p in range(PIECES)]
        self.tokens, self.first = [], []
        for at in parts:
            self.tokens.append(self.start(tok.at[:, at], tok_buf.at[:, at]))
            self.first.append(
                [
                    self.start(ref.at[g, at, :], buf.at[at, pl.ds(n * LANES, LANES)])
                    for n, (ref, g) in enumerate(weights[:2])
                ]
            )
        self.table_copies = [
            self.start(far.at[pl.ds(lax.axis_index("sp"), 1), :], row_buf),
            self.start(near, near_buf),
        ]
        self.later = [
            self.start(ref.at[g], buf.at[:, pl.ds(n * LANES, LANES)])
            for n, (ref, g) in enumerate(weights[2:], 2)
        ]

    def start(self, source, target):
        copy = pltpu.make_async_copy(source, target, self.sem.at[self.used])
        copy.start()
        self.used += 1
        return copy

    def tables(self):
        for copy in self.table_copies:
            copy.wait()
        return turn_tables(self.row_buf[...], self.near_buf)

    def first_pair(self):
        total = None
        width = self.tok_buf.shape[1] // PIECES
        for p in range(PIECES):
            self.tokens[p].wait()
            for copy in self.first[p]:
                copy.wait()
            at = pl.ds(p * width, width)
            part = jnp.dot(
                self.tok_buf[:, at], self.buf[at, : 2 * LANES], preferred_element_type=F32
            )
            total = part if total is None else total + part
        return total

    def product(self, n, count):
        for m in range(count):
            self.later[n - 2 + m].wait()
        return jnp.dot(
            self.tok_buf[...], self.buf[:, pl.ds(n * LANES, count * LANES)],
            preferred_element_type=F32,
        )


def projector_scratch(length, width, weights):
    return [
        pltpu.VMEM((length, width), BF),
        pltpu.VMEM((width, weights * LANES), BF),
        pltpu.VMEM((1, 4 * LANES), F32),
        pltpu.VMEM((2, length, LANES), F32),
        pltpu.SemaphoreType.DMA((3 * PIECES + weights,)),
    ]


def far_kernel(tok, wk, wv, far, near, out, scratch, *buffers):
    work = Projector(tok, ((wk, 2), (wv, 2)), far, near, *buffers)
    both = work.first_pair()
    store_by_class(both[:, LANES:], scratch.at[1], out.at[1], FAR)
    store_by_class(rotate(both[:, :LANES], work.tables()), scratch.at[0], out.at[0], FAR)


def edges_kernel(tok, wq, wk, wv, far, near, q3, kv1, up, down, scratch, *buffers):
    length = tok.shape[0]
    weights = ((wk, 1), (wv, 1), (wk, 0), (wv, 0), (wq, 2))
    work = Projector(tok, weights, far, near, *buffers)
    both = work.first_pair()
    tables = work.tables()
    rows = length // MIDDLE
    for n, x2 in enumerate((rotate(both[:, :LANES], tables), both[:, LANES:])):
        scratch[n] = x2
        for c in range(MIDDLE):
            part = scratch[n, pl.ds(c, rows, stride=MIDDLE), :].astype(BF)
            up[n, pl.ds(c * rows, rows), :] = part
            down[n, pl.ds(c * rows, rows), :] = part
    both = work.product(2, 2)
    for n, x1 in enumerate((rotate(both[:, :LANES], tables), both[:, LANES:])):
        x1 = x1.astype(BF)
        kv1[n] = x1
        up[n, pl.ds(length, SIDE), :] = x1[length - SIDE :]
        down[n, pl.ds(length, SIDE), :] = x1[:SIDE]
    store_by_class(rotate(work.product(4, 1), tables), scratch.at[2], q3, FAR)


def pack_kernel(q3, kv3, halo3, packed):
    size = packed.shape[1] // 5
    for y in range(ROW):
        at = pl.ds(y * size, size)
        for n, part in enumerate((q3[at, :], kv3[0, at, :], kv3[1, at, :], halo3[0, at, :], halo3[1, at, :])):
            packed[SLOT[y], pl.ds(n * size, size), :] = part


def attend(q, k, v, low, high):
    n, keys = q.shape[0], k.shape[0]
    lane = lax.broadcasted_iota(jnp.int32, (1, LANES), 1)
    first = (lane < HEAD_DIM).astype(F32).astype(BF)
    second = (lane >= HEAD_DIM).astype(F32).astype(BF)
    both = jnp.concatenate([q * first, q * second], axis=0)
    scores = lax.dot_general(both, k, (((1,), (1,)), ((), ())), preferred_element_type=F32)
    scores = scores * HEAD_DIM ** (-0.5)
    column = lax.broadcasted_iota(jnp.int32, (n, keys), 1)
    relative = column - lax.broadcasted_iota(jnp.int32, (n, keys), 0)
    allowed = (relative >= 0) & (relative <= 2 * SIDE) & (column >= low) & (column < high)
    outs, tops, sums = [], [], []
    for head in range(2):
        part = jnp.where(allowed, scores[head * n : (head + 1) * n], -1e30)
        top = jnp.max(part, axis=-1, keepdims=True)
        expo = jnp.exp(part - top)
        sums.append(jnp.sum(expo, axis=-1, keepdims=True))
        tops.append(top)
        outs.append(jnp.dot(expo.astype(BF), v, preferred_element_type=F32))
    is_first = lax.broadcasted_iota(jnp.int32, (n, LANES), 1) < HEAD_DIM
    denom = jnp.where(is_first, sums[0], sums[1])
    lse = [t + jnp.log(d) for t, d in zip(tops, sums)]
    return jnp.where(is_first, outs[0], outs[1]) / denom, lse


def spread(lse, rows):
    return jnp.where(lax.broadcasted_iota(jnp.int32, (rows, LANES), 1) < HEAD_DIM, lse[0], lse[1])


def merge(out_a, lse_a, out_b, lse_b):
    top = jnp.maximum(lse_a, lse_b)
    wa, wb = jnp.exp(lse_a - top), jnp.exp(lse_b - top)
    total = wa + wb
    return (wa * out_a + wb * out_b) / total, top + jnp.log(total)


def near_attention_kernel(
    devices, tok, wq, far, near, kv1, up, low, high, out, lse, out2, lse2, q12, scratch, *buffers
):
    length = kv1.shape[1]
    work = Projector(tok, ((wq, 0), (wq, 1)), far, near, *buffers)
    both = work.first_pair()
    tables = work.tables()
    q12[0] = rotate(both[:, :LANES], tables).astype(BF)
    store_by_class(rotate(both[:, LANES:], tables), scratch, q12.at[1], MIDDLE)
    me = lax.axis_index("sp")
    rows = length // MIDDLE
    start = jnp.where(me == 0, SIDE, 0)
    for c in range(MIDDLE):
        at = pl.ds(c * rows, rows)
        k = jnp.concatenate([low[0, at, :], up[0, at, :], high[0, at, :]], axis=0)
        v = jnp.concatenate([low[1, at, :], up[1, at, :], high[1, at, :]], axis=0)
        o, l = attend(
            q12[1, at, :], k, v, start, jnp.where(me == devices - 1, 2 * rows, 3 * rows)
        )
        out2[pl.ds(c, rows, stride=MIDDLE), :] = o
        lse2[pl.ds(c, rows, stride=MIDDLE), :] = spread(l, rows)
    block = 2 * SIDE
    for b in range(length // block):
        ks, vs = [], []
        for n, xs in enumerate((ks, vs)):
            if b == 0:
                xs.append(low[n, pl.ds(length, SIDE), :])
            first = max(b * block - SIDE, 0)
            last = min((b + 1) * block + SIDE, length)
            xs.append(kv1[n, pl.ds(first, last - first), :])
            if b == length // block - 1:
                xs.append(high[n, pl.ds(length, SIDE), :])
        at = pl.ds(b * block, block)
        o, l = attend(
            q12[0, at, :],
            jnp.concatenate(ks, axis=0),
            jnp.concatenate(vs, axis=0),
            start if b == 0 else 0,
            jnp.where(me == devices - 1, block + SIDE, 2 * block)
            if b == length // block - 1
            else 2 * block,
        )
        out[at, :], lse[at, :] = merge(
            o, spread(l, block), out2[at, :], lse2[at, :]
        )


def far_attention_kernel(rows_of_devices, parts, out):
    z = lax.axis_index("sp") // ROW
    low = jnp.where(z == 0, SIDE, 0)
    size = parts.shape[1] // 5
    run = size // 2
    half = ROW // 2
    queries = ROW * run
    high = jnp.where(z == rows_of_devices - 1, queries + SIDE, queries + 2 * SIDE)
    lane = lax.broadcasted_iota(jnp.int32, (queries, LANES), 1)
    group = lax.broadcasted_iota(jnp.int32, (FOLD, LANES), 1) // (LANES // 4)
    which = lane // (LANES // 16) % 4
    folded = [jnp.zeros((FOLD, LANES), F32) for _ in range(ROW)]
    for e in range(2):
        piece = lambda a, y: parts[SLOT[y], pl.ds(a * size + e * run, run), :]
        q = jnp.concatenate([piece(0, y) for y in range(ROW)], axis=0)
        kv = [
            jnp.concatenate(
                [piece(a + 2, y) for y in range(half, ROW)]
                + [piece(a, y) for y in range(ROW)]
                + [piece(a + 2, y) for y in range(half)],
                axis=0,
            )
            for a in (1, 2)
        ]
        o, l = attend(q, kv[0], kv[1], low, high)
        coarse = [x.astype(BF).astype(F32) for x in l]
        fine = [x - c for x, c in zip(l, coarse)]
        terms = jnp.where(
            which < 2,
            jnp.where(which == 0, coarse[0], fine[0]),
            jnp.where(which == 2, coarse[1], fine[1]),
        )
        o = o.astype(BF)
        for y in range(ROW):
            out[SLOT[y], pl.ds(e * run, run), :] = o[y * run : (y + 1) * run]
            for h in range(2):
                at = y * run + h * FOLD
                folded[y] = jnp.where(group == 2 * e + h, terms[at : at + FOLD], folded[y])
    for y in range(ROW):
        out[SLOT[y], pl.ds(size, FOLD), :] = folded[y].astype(BF)


def merge_kernel(parts, out12, lse12, merged, out3, lse3):
    run = merged.shape[1] // FAR
    size = 2 * run
    quarter, eighth = LANES // 4, LANES // 8
    for y in range(ROW):
        terms = parts[SLOT[y], pl.ds(size, FOLD), :].astype(F32)
        total = terms + pltpu.roll(terms, LANES - LANES // 16, 1)
        for e in range(2):
            at = pl.ds(2 * y + e, run, stride=FAR)
            out3[at, :] = parts[SLOT[y], pl.ds(e * run, run), :].astype(F32)
            rows = []
            for h in range(2):
                n = (2 * e + h) * quarter
                rows.append(spread((total[:, n : n + 1], total[:, n + eighth : n + eighth + 1]), FOLD))
            lse3[at, :] = jnp.concatenate(rows, axis=0)
    o, _ = merge(out12[...], lse12[...], out3[...], lse3[...])
    o = o.astype(BF)
    for n in range(merged.shape[0]):
        merged[n] = o


def output_kernel(gathered, weight, mixed):
    total = None
    columns = gathered.shape[3]
    for at, n in enumerate(CHIPS):
        pair = jnp.concatenate([gathered[0, at], gathered[1, at]], axis=1)
        part = jnp.dot(
            pair, weight[pl.ds(2 * n * columns, 2 * columns), :], preferred_element_type=F32
        )
        total = part if total is None else total + part
    mixed[...] = total.astype(BF)


def vmem(shape):
    return jax.ShapeDtypeStruct(shape, BF)


def whole():
    return pl.BlockSpec(memory_space=pltpu.VMEM)


def room(mib):
    return pltpu.CompilerParams(vmem_limit_bytes=int(mib * 1024) << 10)


def cost(flops, size):
    return pl.CostEstimate(flops=flops, bytes_accessed=size, transcendentals=0)


def per_device(devices, tokens, query_weight, key_weight, value_weight, out_weight):
    length, width = tokens.shape
    columns = key_weight.shape[2]
    far, near = rotary_tables(devices, length)
    stay = functools.partial(pltpu.with_memory_space_constraint, memory_space=pltpu.HBM)
    tokens, query_weight, key_weight, value_weight, far, near = (
        stay(x) for x in (tokens, query_weight, key_weight, value_weight, jnp.asarray(far), jnp.asarray(near))
    )
    hbm = pl.BlockSpec(memory_space=pltpu.HBM)
    flat = jax.ShapeDtypeStruct((length, columns), F32)
    scratch = pltpu.VMEM((length, columns), F32)
    kv3 = pl.pallas_call(
        far_kernel,
        in_specs=[hbm] * 5,
        out_specs=whole(),
        out_shape=vmem((2, length, columns)),
        scratch_shapes=[pltpu.VMEM((2, length, columns), F32)]
        + projector_scratch(length, width, 2),
        cost_estimate=cost(4 * length * width * columns, 2 << 20),
        compiler_params=room(GRANT),
        name="far_keys_values",
    )(tokens, key_weight, value_weight, far, near)

    half = ROW // 2
    route = []
    for s in range(devices):
        target = s + ROW if s % ROW >= half else s - ROW
        if 0 <= target < devices:
            route.append((s, target))
    halo3 = lax.ppermute(kv3, "sp", route)

    edge = length + SIDE
    shapes = [
        (length, columns),
        (2, length, columns),
        (2, edge, columns),
        (2, edge, columns),
    ]
    q3, kv1, up, down = pl.pallas_call(
        edges_kernel,
        in_specs=[hbm] * 6,
        out_specs=[whole()] * len(shapes),
        out_shape=[vmem(s) for s in shapes],
        scratch_shapes=[pltpu.VMEM((3, length, columns), F32)]
        + projector_scratch(length, width, 5),
        cost_estimate=cost(10 * length * width * columns, 4 << 20),
        compiler_params=room(GRANT),
        name="projections",
    )(tokens, query_weight, key_weight, value_weight, far, near)

    low = lax.ppermute(up, "sp", [(s, s + 1) for s in range(devices - 1)])
    high = lax.ppermute(down, "sp", [(s + 1, s) for s in range(devices - 1)])

    size = length // ROW
    packed = pl.pallas_call(
        pack_kernel,
        in_specs=[whole()] * 3,
        out_specs=whole(),
        out_shape=vmem((ROW, 5 * size, columns)),
        cost_estimate=cost(1 << 20, 1 << 19),
        compiler_params=room(2),
        name="pack",
    )(q3, kv3, halo3)
    groups = [[z * ROW + y for y in ORDER] for z in range(devices // ROW)]
    parts = lax.all_to_all(packed, "sp", 0, 0, axis_index_groups=groups, tiled=True)

    back = pl.pallas_call(
        functools.partial(far_attention_kernel, devices // ROW),
        in_specs=[whole()],
        out_specs=whole(),
        out_shape=vmem((ROW, size + FOLD, columns)),
        cost_estimate=cost(1 << 27, 1 << 19),
        compiler_params=room(4),
        name="far_attention",
    )(parts)
    parts3 = lax.all_to_all(back, "sp", 0, 0, axis_index_groups=groups, tiled=True)

    out12, lse12 = pl.pallas_call(
        functools.partial(near_attention_kernel, devices),
        in_specs=[hbm] * 4 + [whole()] * 4,
        out_specs=[whole()] * 2,
        out_shape=[flat, flat],
        scratch_shapes=[scratch, scratch, pltpu.VMEM((2, length, columns), BF), scratch]
        + projector_scratch(length, width, 2),
        cost_estimate=cost(1 << 28, 1 << 20),
        compiler_params=room(GRANT),
        name="near_attention",
    )(tokens, query_weight, far, near, kv1, up, low, high)

    chips = lax.axis_size("tp") // 2
    merged = pl.pallas_call(
        merge_kernel,
        in_specs=[whole()] * 3,
        out_specs=whole(),
        out_shape=vmem((chips, length, columns)),
        scratch_shapes=[scratch, scratch],
        cost_estimate=cost(1 << 20, 1 << 19),
        compiler_params=room(2),
        name="merge",
    )(parts3, out12, lse12)

    lines = [[2 * n + core for n in CHIPS] for core in range(2)]
    gathered = lax.all_to_all(merged, "tp", 0, 0, axis_index_groups=lines, tiled=True)
    cores = [[2 * n, 2 * n + 1] for n in range(chips)]
    gathered = lax.all_gather(gathered, "tp", axis=0, axis_index_groups=cores)
    return pl.pallas_call(
        output_kernel,
        in_specs=[whole()] * 2,
        out_specs=whole(),
        out_shape=vmem((length, out_weight.shape[1])),
        cost_estimate=cost(1 << 27, 1 << 20),
        compiler_params=room(4),
        name="output",
    )(gathered, out_weight)


def solution(mesh):
    weights = P(None, None, "tp")

    def body(*args):
        return per_device(mesh.shape["sp"], *args)

    return jax.shard_map(
        body,
        mesh=mesh,
        in_specs=(P("sp", None), weights, weights, weights, P(None, "tp")),
        out_specs=P("sp", "tp"),
        check_vma=False,
    )
```
